32 devices in a mesh: sp: 8 (over z, y), tp: 4 (over x, core).
Axes of the slice: x: 2, y: 2, z: 4, core: 2. Of those that a mesh axis runs over, the one named last changes fastest.
Arguments:
- residual_input_stream: bfloat16 [8192, 2048], P(('sp', 'tp')), may hold values from -6 to 6
- receptance: bfloat16 [8192, 1024], P('sp', 'tp'), may hold values from -6 to 6
- key_matrix_all: bfloat16 [8192, 1024], P('sp', 'tp'), may hold values from -6 to 6
- value_matrix_all: bfloat16 [8192, 1024], P('sp', 'tp'), may hold values from -6 to 6
- decay_preactivation: bfloat16 [8192, 1024], P('sp', 'tp'), may hold values from -15 to 1
- learning_rate_preactivation: bfloat16 [8192, 1024], P('sp', 'tp'), may hold values from -11 to 5
- output_gate_all_heads: bfloat16 [8192, 1024], P('sp', 'tp'), may hold values from -6 to 6
- extra_log_decay: float32 [8192, 1024], P('sp', 'tp'), may hold values from -0.7 to 0
- head_norm_gain: float32 [1024], P('tp'), may hold values from 0.1 to 1.9
- output_projection_weight: bfloat16 [1024, 2048], P('tp'), may hold values from -0.1875 to 0.1875
- feedforward_norm_gain: float32 [2048], replicated, may hold values from 0.1 to 1.9
- gate_projection_weight: bfloat16 [2048, 5632], P('sp', 'tp'), may hold values from -0.125 to 0.125
- up_projection_weight: bfloat16 [2048, 5632], P('sp', 'tp'), may hold values from -0.125 to 0.125
- down_projection_weight: bfloat16 [2048, 5632], P('sp', 'tp'), may hold values from -0.078125 to 0.078125
- convolution_kernel: bfloat16 [3, 2, 5632], P(None, None, 'tp'), may hold values from -3.5 to 3.5
Outputs:
- layer_out: bfloat16 [8192, 2048], P(('sp', 'tp'))
The draws below stay inside these ranges and needn't reach their ends.
All inputs are finite; a program needn't handle non-finite values.
Results may differ from the reference program's by a relative error of at most 0.022.
Values may be sent and summed in bfloat16 or wider, within the bound.
A program may use at most 128 MiB of HBM per device.

```python
import math
import jax
import jax.numpy as jnp
from jax import lax

D = 2048
HEAD_TOTAL = 16
HEAD_WIDTH = 64
FF = 5632
TOK_DEV = 1024
TOKEN_TOTAL = 8192
N_TP = 4


def slow_heads(key):
    share = 0.5
    return jax.random.uniform(jax.random.fold_in(key, 7), (HEAD_TOTAL,)) < share


def head_noise(key, scale):
    return scale * jax.random.truncated_normal(key, -4.0, 4.0, (TOKEN_TOTAL, HEAD_TOTAL * HEAD_WIDTH), jnp.float32)


def draw_decay_preactivation(key, part):
    slow = slow_heads(key)
    base = jnp.repeat(jnp.where(slow, -10.5, -3.2), HEAD_WIDTH)
    noise = head_noise(jax.random.fold_in(key, 1), 0.8)
    offsets = jax.random.uniform(jax.random.fold_in(key, 2), (TOKEN_TOTAL // TOK_DEV, 1), jnp.float32, -0.8, 0.8)
    return (base[None, :] + noise + jnp.repeat(offsets, TOK_DEV, axis=0)).astype(jnp.bfloat16)


def draw_learning_rate_preactivation(key, part):
    slow = slow_heads(key)
    base = jnp.repeat(jnp.where(slow, -6.5, 0.5), HEAD_WIDTH)
    noise = head_noise(jax.random.fold_in(key, 3), 1.0)
    return (base[None, :] + noise).astype(jnp.bfloat16)


def draw_extra_log_decay(key, part):
    hits = jax.random.uniform(jax.random.fold_in(key, 4), (TOKEN_TOTAL, HEAD_TOTAL)) < 4.0 / TOKEN_TOTAL
    values = jax.random.uniform(jax.random.fold_in(key, 5), (TOKEN_TOTAL, HEAD_TOTAL * HEAD_WIDTH), jnp.float32, math.log(0.5), math.log(0.8))
    return jnp.where(jnp.repeat(hits, HEAD_WIDTH, axis=1), values, 0.0)


def level_of(own_key, shape, shards, least, high):
    def one(axis_at, parts):
        draws = jax.random.uniform(jax.random.fold_in(jax.random.fold_in(own_key, 6), axis_at), (parts,), jnp.float32, least / len(shards), high / len(shards))
        return jnp.repeat(jnp.exp(draws), shape[axis_at] // parts).reshape((-1,) + (1,) * (len(shape) - axis_at - 1))

    level = one(*shards[0])
    for cut in shards[1:]:
        level = level * one(*cut)
    return level


def scatter_about(key, shape, scale, bound, shards=(), dtype=jnp.bfloat16):
    array = scale * jax.random.normal(key, shape, jnp.float32)
    if shards:
        array = array * level_of(key, shape, shards, -0.22, 0.18)
    return jnp.clip(array, -bound, bound).astype(dtype)


def setup_inputs(seed: int = 0) -> dict:
    streams_of = jax.random.split(jax.random.key(seed), 16)
    return {
        "residual_input_stream": scatter_about(streams_of[0], (TOKEN_TOTAL, D), 1.0, 6.0, ((0, 32),)),
        "receptance": scatter_about(streams_of[1], (TOKEN_TOTAL, HEAD_TOTAL * HEAD_WIDTH), 1.0, 6.0, ((0, 8), (1, 4))),
        "key_matrix_all": scatter_about(streams_of[2], (TOKEN_TOTAL, HEAD_TOTAL * HEAD_WIDTH), 1.0, 6.0, ((0, 8), (1, 4))),
        "value_matrix_all": scatter_about(streams_of[3], (TOKEN_TOTAL, HEAD_TOTAL * HEAD_WIDTH), 1.0, 6.0, ((0, 8), (1, 4))),
        "decay_preactivation": draw_decay_preactivation(jax.random.fold_in(streams_of[15], 71), 0),
        "learning_rate_preactivation": draw_learning_rate_preactivation(jax.random.fold_in(streams_of[15], 71), 0),
        "output_gate_all_heads": scatter_about(streams_of[6], (TOKEN_TOTAL, HEAD_TOTAL * HEAD_WIDTH), 1.0, 6.0, ((0, 8), (1, 4))),
        "extra_log_decay": draw_extra_log_decay(jax.random.fold_in(streams_of[15], 71), 0),
        "head_norm_gain": jnp.clip(1.0 + 0.18 * jax.random.normal(streams_of[8], (HEAD_TOTAL * HEAD_WIDTH,), jnp.float32), 0.1, 1.9),
        "output_projection_weight": scatter_about(streams_of[9], (HEAD_TOTAL * HEAD_WIDTH, D), (HEAD_TOTAL * HEAD_WIDTH) ** -0.5, 0.1875, ((0, 4),)),
        "feedforward_norm_gain": jnp.clip(1.0 + 0.18 * jax.random.normal(streams_of[10], (D,), jnp.float32), 0.1, 1.9),
        "gate_projection_weight": scatter_about(streams_of[11], (D, FF), D ** -0.5, 0.125, ((0, 8), (1, 4))),
        "up_projection_weight": scatter_about(streams_of[12], (D, FF), D ** -0.5, 0.125, ((0, 8), (1, 4))),
        "down_projection_weight": scatter_about(streams_of[13], (D, FF), FF ** -0.5, 0.078125, ((0, 8), (1, 4))),
        "convolution_kernel": scatter_about(streams_of[14], (3, 2, FF), 0.577, 3.5, ((2, 4),)),
    }


highest = lax.Precision.HIGHEST

def per_head_layout(values_in):
    return values_in.astype(jnp.float32).reshape(values_in.shape[0], HEAD_TOTAL, HEAD_WIDTH)

def reference(residual_input_stream, receptance, key_matrix_all, value_matrix_all, decay_preactivation, learning_rate_preactivation, output_gate_all_heads, extra_log_decay, head_norm_gain, output_projection_weight, feedforward_norm_gain, gate_projection_weight, up_projection_weight, down_projection_weight, convolution_kernel):
    queries = per_head_layout(receptance)
    keys = per_head_layout(key_matrix_all)
    values = per_head_layout(value_matrix_all)
    decay_logarithm = -jnp.exp(-jax.nn.softplus(-per_head_layout(decay_preactivation)) - 0.5) + extra_log_decay.reshape(TOKEN_TOTAL, HEAD_TOTAL, HEAD_WIDTH)
    factors = jnp.exp(decay_logarithm)
    rates = jax.nn.sigmoid(per_head_layout(learning_rate_preactivation))
    normed_keys = keys * lax.rsqrt(lax.optimization_barrier(jnp.sum(keys * keys, axis=-1, keepdims=True)) + 1e-06)
    removal = normed_keys * rates

    def advance(carried, inputs_now):
        query_now, key_now, value_now, factor_now, normed_now, removal_now = inputs_now
        along = jnp.einsum('hvk,hk->hv', carried, normed_now, precision=highest)
        carried = carried * factor_now[:, None, :] - along[:, :, None] * removal_now[:, None, :] + value_now[:, :, None] * key_now[:, None, :]
        return (carried, jnp.einsum('hvk,hk->hv', carried, query_now, precision=highest))
    start_state = jnp.zeros((HEAD_TOTAL, HEAD_WIDTH, HEAD_WIDTH), jnp.float32)
    final_state, readout = lax.scan(advance, start_state, (queries, keys, values, factors, normed_keys, removal))
    centered = readout - lax.optimization_barrier(jnp.mean(readout, axis=-1, keepdims=True))
    variance = lax.optimization_barrier(jnp.mean(centered * centered, axis=-1, keepdims=True))
    normalized = (centered * lax.rsqrt(variance + 0.00064)).reshape(TOKEN_TOTAL, HEAD_TOTAL * HEAD_WIDTH)
    mixed_out = (normalized * head_norm_gain * output_gate_all_heads.astype(jnp.float32)).astype(jnp.bfloat16)
    group_width = HEAD_TOTAL * HEAD_WIDTH // N_TP
    attention = jnp.zeros((TOKEN_TOTAL, D), jnp.float32)
    for group in range(N_TP):
        part = jnp.dot(mixed_out[:, group * group_width:(group + 1) * group_width], output_projection_weight[group * group_width:(group + 1) * group_width], preferred_element_type=jnp.float32)
        attention = attention + lax.optimization_barrier(part.astype(jnp.bfloat16)).astype(jnp.float32)
    stream = lax.optimization_barrier((residual_input_stream.astype(jnp.float32) + attention).astype(jnp.bfloat16))
    stream_wide = stream.astype(jnp.float32)
    normed = (stream_wide * lax.rsqrt(lax.optimization_barrier(jnp.mean(stream_wide * stream_wide, axis=-1, keepdims=True)) + 1e-06) * feedforward_norm_gain).astype(jnp.bfloat16)
    taps = convolution_kernel.astype(jnp.float32)
    unit_width = FF // N_TP
    block_count = TOKEN_TOTAL // TOK_DEV

    def ffn_block(carried, inputs_now):
        normed_block, stream_block = inputs_now
        gate_pre = jnp.dot(normed_block, gate_projection_weight, preferred_element_type=jnp.float32).astype(jnp.bfloat16)
        up_pre = jnp.dot(normed_block, up_projection_weight, preferred_element_type=jnp.float32).astype(jnp.bfloat16)
        gate_ext = jnp.concatenate([carried[0], gate_pre], axis=0).astype(jnp.float32)
        up_ext = jnp.concatenate([carried[1], up_pre], axis=0).astype(jnp.float32)
        gate_mix = taps[0, 0] * gate_ext[:-2] + taps[1, 0] * gate_ext[1:-1] + taps[2, 0] * gate_ext[2:]
        up_mix = taps[0, 1] * up_ext[:-2] + taps[1, 1] * up_ext[1:-1] + taps[2, 1] * up_ext[2:]
        hidden = (jax.nn.silu(gate_mix) * up_mix).astype(jnp.bfloat16)
        ffn = jnp.zeros((TOK_DEV, D), jnp.float32)
        for group in range(N_TP):
            part = jnp.dot(hidden[:, group * unit_width:(group + 1) * unit_width], down_projection_weight[:, group * unit_width:(group + 1) * unit_width].T, preferred_element_type=jnp.float32)
            ffn = ffn + lax.optimization_barrier(part.astype(jnp.bfloat16)).astype(jnp.float32)
        layer_block = (stream_block.astype(jnp.float32) + ffn).astype(jnp.bfloat16)
        return ((gate_pre[-2:], up_pre[-2:]), layer_block)
    start_rows = (jnp.zeros((2, FF), jnp.bfloat16), jnp.zeros((2, FF), jnp.bfloat16))
    last_rows, layer_blocks = lax.scan(ffn_block, start_rows, (normed.reshape(block_count, TOK_DEV, D), stream.reshape(block_count, TOK_DEV, D)))
    return layer_blocks.reshape(TOKEN_TOTAL, D)
```

```python
import functools

import jax
import jax.numpy as jnp
from jax import lax
from jax.experimental import pallas as pl
from jax.experimental.pallas import tpu as pltpu
from jax.sharding import PartitionSpec as P

HEAD_WIDTH = 64
BLOCK = 64
PER_STEP = 4
HALO = 16
LAG = 3
MESH = pl.DeviceIdType.MESH
WIDE = jnp.float32
NARROW = jnp.bfloat16


def mul(a, b, dims=((1,), (0,))):
    return lax.dot_general(
        a.astype(NARROW), b.astype(NARROW), (dims, ((), ())), preferred_element_type=WIDE
    )


def parts_of(a, count):
    found = []
    for _ in range(count):
        piece = a.astype(NARROW)
        found.append(piece)
        a = a - piece.astype(WIDE)
    return found


def fine_left(a, b, count, dims=((1,), (0,))):
    return sum(mul(piece, b, dims) for piece in parts_of(a, count))


def fine_right(a, b, count, dims=((1,), (0,))):
    return sum(mul(a, piece, dims) for piece in parts_of(b, count))


def head_mask(width):
    rows = lax.broadcasted_iota(jnp.int32, (width, width), 0) // HEAD_WIDTH
    lanes = lax.broadcasted_iota(jnp.int32, (width, width), 1) // HEAD_WIDTH
    return jnp.where(rows == lanes, 1.0, 0.0)


def stacked(a, mask):
    a = a.astype(NARROW)
    return jnp.concatenate([a] * (mask.shape[0] // a.shape[0]), axis=0) * mask


def fine_product(a, b, mask):
    a_high, a_low = parts_of(a, 2)
    b_high, b_low = (stacked(piece, mask) for piece in parts_of(b, 2))
    return mul(a_high, b_high) + mul(a_low, b_high) + mul(a_high, b_low)


def collapsed(a):
    heads = a.shape[0] // HEAD_WIDTH
    return sum(a[h * HEAD_WIDTH : (h + 1) * HEAD_WIDTH] for h in range(heads))


def recurrence(refs, local_ref, reach_ref, state, before_step):
    q_ref, k_ref, v_ref, decay_ref, rate_ref, extra_ref = refs
    tokens, width = q_ref.shape
    mask_wide = head_mask(width)
    mask = mask_wide.astype(NARROW)
    last = ((1,), (1,))
    first = ((0,), (0,))

    rows = lax.broadcasted_iota(jnp.int32, (width, width), 0)
    lanes = lax.broadcasted_iota(jnp.int32, (width, width), 1)
    state[:, :width] = jnp.zeros((width, width), WIDE)
    state[:, width:] = jnp.where(rows == lanes, 1.0, 0.0)

    def one(index, carry):
        before_step(index)
        token = lax.broadcasted_iota(jnp.int32, (BLOCK, width), 0)
        other = lax.broadcasted_iota(jnp.int32, (BLOCK, width), 1) % BLOCK
        strict = token > other
        within = token >= other
        eye = jnp.where(token == other, 1.0, 0.0)
        lower = jnp.where(
            lax.broadcasted_iota(jnp.int32, (BLOCK, BLOCK), 0)
            >= lax.broadcasted_iota(jnp.int32, (BLOCK, BLOCK), 1),
            1.0,
            0.0,
        ).astype(NARROW)
        ones = jnp.ones((BLOCK, width), NARROW)

        def window(part):
            return pl.ds(pl.multiple_of((index * PER_STEP + part) * BLOCK, BLOCK), BLOCK)

        prepared = []
        for part in range(PER_STEP):
            at = window(part)
            q = q_ref[at].astype(WIDE)
            k = k_ref[at].astype(WIDE)
            v = stacked(v_ref[at], mask)
            log_decay = (
                -jnp.exp(-0.5) * jax.nn.sigmoid(decay_ref[at].astype(WIDE)) + extra_ref[at]
            )
            rates = jax.nn.sigmoid(rate_ref[at].astype(WIDE))
            normed = k * lax.rsqrt(fine_left(k * k, mask, 2) + 1e-06)
            removal = normed * rates
            cum = fine_right(lower, log_decay, 3)
            previous = cum - log_decay
            middle = cum[BLOCK // 2 : BLOCK // 2 + 1]
            end = cum[BLOCK - 1 : BLOCK]
            back = jnp.exp(middle - cum)
            left = jnp.concatenate(
                [normed * jnp.exp(previous - middle), q * jnp.exp(cum - middle)], axis=0
            )
            by_key = mul(left, stacked(k * back, mask), last)
            by_removal = mul(left, stacked(removal * back, mask), last)
            key_rate = jnp.where(strict, by_key[:BLOCK], 0.0)
            removal_rate = jnp.where(strict, by_removal[:BLOCK], 0.0)
            key_out = jnp.where(within, by_key[BLOCK:], 0.0)
            removal_out = jnp.where(within, by_removal[BLOCK:], 0.0)
            inverse = eye
            size = 1
            while size < BLOCK:
                pair = (token // (2 * size) == other // (2 * size)) & (
                    token // size != other // size
                )
                piece = jnp.where(pair, removal_rate, 0.0)
                if size == 1:
                    inverse = inverse - piece
                else:
                    inverse = inverse - fine_product(
                        fine_product(inverse, piece, mask), inverse, mask
                    )
                size *= 2
            from_state = mul(inverse, stacked(normed * jnp.exp(previous), mask))
            keyed = mul(jnp.concatenate([key_rate, key_out], axis=0), v)
            offset = mul(inverse, stacked(keyed[:BLOCK], mask))
            reach = q * jnp.exp(cum) - mul(removal_out, stacked(from_state, mask))
            local = keyed[BLOCK:] - mul(removal_out, stacked(offset, mask))
            to_end = jnp.exp(end - cum)
            span = jnp.exp(fine_left(log_decay, ones, 3, first))
            prepared.append((from_state, offset, reach, local, k * to_end, removal * to_end, span))

        for part in range(PER_STEP):
            at = window(part)
            from_state, offset, reach, local, key_end, removal_end, span = prepared[part]
            now = state[...]
            both = mul(jnp.concatenate([from_state, reach], axis=0), now)
            correction = both[:BLOCK, :width] + offset
            local_ref[at] = local + both[BLOCK:, :width]
            reach_ref[at] = both[BLOCK:, width:]
            kept_value = mul(
                jnp.concatenate([key_end, -removal_end], axis=0),
                jnp.concatenate([v_ref[at].astype(WIDE), correction], axis=0),
                first,
            )
            kept_map = mul(-removal_end, both[:BLOCK, width:], first)
            state[:, :width] = now[:, :width] * span + kept_value * mask_wide
            state[:, width:] = now[:, width:] * span + kept_map * mask_wide
        return carry

    lax.fori_loop(0, tokens // (BLOCK * PER_STEP), one, 0)


def ring_plan(count):
    hops = count // 2

    def entries(weight, hop):
        if hop < hops - 1:
            return [(weight, 0, hop), (weight, 1, hop)]
        return [(weight, None, hop)]

    plan = []
    for weight in range(3):
        plan += entries(weight, 0)
    for hop in range(1, hops):
        plan += entries(0, hop) + entries(1, hop)
    for hop in range(1, hops):
        plan += entries(2, hop)
    return plan


class Ring:
    def __init__(self, axis, shards, gathered, sems):
        self.axis, self.shards, self.gathered, self.sems = axis, shards, gathered, sems
        self.count = lax.axis_size(axis)
        me = lax.axis_index(axis)
        odd = lax.rem(me, 2)
        self.place = (1 - odd) * (me // 2) + odd * (self.count - 1 - me // 2)
        self.plan = ring_plan(self.count)
        self.number = {}
        for at, (weight, half, hop) in enumerate(self.plan):
            for way in (0, 1):
                self.number[weight, way if half is None else half, hop, way] = at
        self.issued = 0
        self.waited = set()

    def index(self, offset):
        at = lax.rem(self.place + offset + 2 * self.count, self.count)
        upper = at // (self.count // 2)
        return (1 - upper) * 2 * at + upper * (2 * (self.count - 1 - at) + 1)

    def block(self, weight, half, offset):
        rows = self.shards[weight].shape[0]
        start = self.index(offset) * rows + half * (rows // 2)
        return self.gathered[weight].at[pl.ds(pl.multiple_of(start, rows // 2), rows // 2)]

    def copy(self, at, way):
        weight, half, hop = self.plan[at]
        half = way if half is None else half
        rows = self.shards[weight].shape[0] // 2
        back = -hop if way == 0 else hop
        target = self.block(weight, half, back)
        source = self.shards[weight].at[pl.ds(half * rows, rows)] if hop == 0 else target
        slot = 2 * at + way
        return pltpu.make_async_remote_copy(
            src_ref=source,
            dst_ref=target,
            send_sem=self.sems[0].at[slot],
            recv_sem=self.sems[1].at[slot],
            device_id={self.axis: self.index(1 if way == 0 else -1)},
            device_id_type=MESH,
        )

    def arrive(self, weight, half, hop, way):
        at = self.number[weight, half, hop, way]
        if (at, way) not in self.waited:
            self.waited.add((at, way))
            self.copy(at, way).wait_recv()

    def issue_to(self, target):
        while self.issued < min(target, len(self.plan)):
            weight, half, hop = self.plan[self.issued]
            for way in (0, 1):
                if hop > 0:
                    self.arrive(weight, way if half is None else half, hop - 1, way)
                self.copy(self.issued, way).start()
            self.issued += 1

    def issue_share(self, numerator, denominator):
        self.issue_to(len(self.plan) * numerator // denominator)

    def issue_through(self, weight, hop):
        while any(w == weight and h <= hop for w, _, h in self.plan[self.issued :]):
            self.issue_to(self.issued + 1)

    def arrive_hop(self, weight, hop, way):
        for half in (0, 1):
            if (weight, half, hop, way) in self.number:
                self.arrive(weight, half, hop, way)

    def arrive_all(self, weight):
        for hop in range(self.count // 2):
            for way in (0, 1):
                self.arrive_hop(weight, hop, way)

    def finish(self):
        for at in range(len(self.plan)):
            for way in (0, 1):
                self.copy(at, way).wait_send()


class Group:
    def __init__(self, axis):
        self.axis = axis
        self.count = lax.axis_size(axis)
        self.me = lax.axis_index(axis)
        self.half = self.count // 2

    def device(self, offset, sibling):
        side = lax.rem(self.me, 2)
        group = lax.rem(self.me // 2 + offset + self.half, self.half)
        return 2 * group + (1 - side if sibling else side)

    def copy(self, source, target, sems, slot, device):
        return pltpu.make_async_remote_copy(
            src_ref=source,
            dst_ref=target,
            send_sem=sems[0].at[slot],
            recv_sem=sems[1].at[slot],
            device_id={self.axis: device},
            device_id_type=MESH,
        )


class Spread:
    def __init__(self, group, source, block, side_sems, far_sems, pass_sems):
        self.group, self.source, self.block = group, source, block
        self.side_sems, self.far_sems, self.pass_sems = side_sems, far_sems, pass_sems
        self.others = range(1, group.half)

    def slot(self, piece, offset):
        return piece * (self.group.half - 1) + offset - 1

    def side(self, piece):
        group = self.group
        return group.copy(
            self.source(piece), self.block(group.me, piece), self.side_sems, piece,
            group.device(0, True),
        )

    def far(self, piece, offset):
        group = self.group
        return group.copy(
            self.source(piece), self.block(group.me, piece), self.far_sems,
            self.slot(piece, offset), group.device(offset, False),
        )

    def onward(self, piece, offset):
        group = self.group
        block = self.block(group.device(-offset, False), piece)
        return group.copy(
            block, block, self.pass_sems, self.slot(piece, offset), group.device(0, True)
        )

    def start(self, piece):
        for offset in self.others:
            self.far(piece, offset).start()
        self.side(piece).start()

    def hand_on(self, piece):
        for offset in self.others:
            self.far(piece, offset).wait_recv()
            self.onward(piece, offset).start()

    def arrive(self, piece):
        self.side(piece).wait_recv()
        for offset in self.others:
            self.onward(piece, offset).wait_recv()

    def finish(self, piece):
        self.side(piece).wait_send()
        for offset in self.others:
            self.far(piece, offset).wait_send()
            self.onward(piece, offset).wait_send()


def layer_kernel(
    q_in, k_in, v_in, decay_in, rate_in, extra_in, out_gate_in, residual_in, out_weight_in,
    gate_in, up_in, down_in, head_gain, ffn_gain, taps,
    out,
    q, k, v, decay, rate, extra, out_gate, local, reach, state, maps,
    stream, out_weight, mixed, normed, full_gate, full_up, full_down, hidden,
    part, near, leaving, far,
    load_sem, ring_send, ring_recv, map_send, map_recv, halo_send, halo_recv,
    rows_side_send, rows_side_recv, rows_far_send, rows_far_recv, rows_pass_send, rows_pass_recv,
    wide_side_send, wide_side_recv, wide_far_send, wide_far_recv, wide_pass_send, wide_pass_recv,
    mix_side_send, mix_side_recv, mix_far_send, mix_far_recv, mix_pass_send, mix_pass_recv,
    near_send, near_recv, far_send, far_recv,
):
    tokens, width = q.shape
    features = stream.shape[1]
    group = Group("tp")
    around = lax.axis_size("sp")
    place = lax.axis_index("sp")
    own_rows = tokens // group.count
    ring = Ring(
        "sp", (gate_in, up_in, down_in), (full_gate, full_up, full_down), (ring_send, ring_recv)
    )
    shard = down_in.shape[0]

    def owned(ref, index, rows):
        return ref.at[pl.ds(pl.multiple_of(index * rows, rows), rows)]

    pairs = list(
        zip(
            (q_in, k_in, v_in, decay_in, rate_in, extra_in, out_gate_in),
            (q, k, v, decay, rate, extra, out_gate),
        )
    )
    inputs = len(pairs)
    pairs += [
        (residual_in, owned(stream, group.me, own_rows)),
        (out_weight_in, owned(out_weight, group.me, width)),
        (gate_in, owned(full_gate, place, shard)),
        (up_in, owned(full_up, place, shard)),
        (down_in, owned(full_down, place, shard)),
    ]
    loads = [
        pltpu.make_async_copy(source, target, load_sem.at[at])
        for at, (source, target) in enumerate(pairs)
    ]
    for load in loads[:inputs]:
        load.start()

    barrier = pltpu.get_barrier_semaphore()
    for axis, count, me in (("sp", around, place), ("tp", group.count, group.me)):
        for step in range(1, count):
            pl.semaphore_signal(
                barrier, inc=1, device_id={axis: lax.rem(me + step, count)}, device_id_type=MESH
            )
    pl.semaphore_wait(barrier, around + group.count - 2)

    ring.issue_share(6, 21)
    rows_spread = Spread(
        group,
        lambda piece: residual_in,
        lambda index, piece: owned(stream, index, own_rows),
        (rows_side_send, rows_side_recv),
        (rows_far_send, rows_far_recv),
        (rows_pass_send, rows_pass_recv),
    )
    wide_spread = Spread(
        group,
        lambda piece: out_weight_in,
        lambda index, piece: owned(out_weight, index, width),
        (wide_side_send, wide_side_recv),
        (wide_far_send, wide_far_recv),
        (wide_pass_send, wide_pass_recv),
    )
    rows_spread.start(0)
    wide_spread.start(0)
    for load in loads[inputs:]:
        load.start()
    for load in loads[:inputs]:
        load.wait()

    def before_step(index):
        @pl.when(index == tokens // (BLOCK * PER_STEP) - 1)
        def _():
            ring.issue_share(8, 21)

    recurrence((q, k, v, decay, rate, extra), local, reach, state, before_step)

    def map_copy(step):
        return pltpu.make_async_remote_copy(
            src_ref=maps.at[place],
            dst_ref=maps.at[place],
            send_sem=map_send.at[step - 1],
            recv_sem=map_recv.at[step - 1],
            device_id={"sp": lax.rem(place + step, around)},
            device_id_type=MESH,
        )

    maps[place] = collapsed(state[...]).astype(NARROW)
    for step in range(1, around):
        map_copy(step).start()
    rows_spread.hand_on(0)
    wide_spread.hand_on(0)
    ring.issue_share(10, 21)
    for step in range(1, around):
        map_copy(step).wait_recv()

    mask = head_mask(width).astype(NARROW)

    def enter(step, entering):
        found = maps[step]
        high, low = parts_of(entering, 2)
        after = (
            found[:, :width].astype(WIDE)
            + mul(found[:, width:], stacked(high, mask))
            + mul(found[:, width:], stacked(low, mask))
        )
        return jnp.where(step < place, after, entering)

    entering = lax.fori_loop(0, around - 1, enter, jnp.zeros((HEAD_WIDTH, width), WIDE))
    state[:, :width] = stacked(entering, mask).astype(WIDE)

    pieces = group.count
    own_lanes = pl.ds(pl.multiple_of(group.me * width, width), width)

    def mixed_block(index, piece):
        rows = pl.ds(pl.multiple_of(piece * own_rows, own_rows), own_rows)
        return mixed.at[rows, pl.ds(pl.multiple_of(index * width, width), width)]

    mix_spread = Spread(
        group,
        lambda piece: mixed_block(group.me, piece),
        mixed_block,
        (mix_side_send, mix_side_recv),
        (mix_far_send, mix_far_recv),
        (mix_pass_send, mix_pass_recv),
    )

    def mix(piece, carry):
        rows = pl.ds(pl.multiple_of(piece * own_rows, own_rows), own_rows)
        readout = local[rows] + mul(reach[rows], state[:, :width])
        centered = readout - fine_left(readout, mask, 2) * (1.0 / HEAD_WIDTH)
        variance = fine_left(centered * centered, mask, 2) * (1.0 / HEAD_WIDTH)
        value = (
            centered
            * lax.rsqrt(variance + 0.00064)
            * head_gain[...]
            * out_gate[rows].astype(WIDE)
        )
        mixed[rows, own_lanes] = value.astype(NARROW)
        mix_spread.start(piece)
        return carry

    lax.fori_loop(0, pieces, mix, 0)
    ring.issue_share(12, 21)
    rows_spread.arrive(0)
    wide_spread.arrive(0)
    rows_spread.finish(0)
    wide_spread.finish(0)
    loads[inputs].wait()
    loads[inputs + 1].wait()

    def settle(piece, carry):
        @pl.when(piece < pieces)
        def _():
            mix_spread.hand_on(piece)

        @pl.when(piece > 0)
        def _():
            done = piece - 1
            mix_spread.arrive(done)
            rows = pl.ds(pl.multiple_of(done * own_rows, own_rows), own_rows)
            total = mul(mixed[rows], out_weight[...])
            kept = (stream[rows].astype(WIDE) + total).astype(NARROW)
            stream[rows] = kept
            kept = kept.astype(WIDE)
            scale = lax.rsqrt(jnp.mean(kept * kept, axis=-1, keepdims=True) + 1e-06)
            after = pl.ds(pl.multiple_of(HALO + done * own_rows, HALO), own_rows)
            normed[after] = (kept * scale * ffn_gain[...]).astype(NARROW)

        return carry

    lax.fori_loop(0, pieces + 1, settle, 0)

    halo = pltpu.make_async_remote_copy(
        src_ref=normed.at[pl.ds(tokens, HALO)],
        dst_ref=normed.at[pl.ds(0, HALO)],
        send_sem=halo_send,
        recv_sem=halo_recv,
        device_id={"sp": lax.rem(place + 1, around)},
        device_id_type=MESH,
    )

    @pl.when(place < around - 1)
    def _():
        halo.start()

    @pl.when(place == 0)
    def _():
        normed[:HALO] = jnp.zeros((HALO, features), NARROW)

    ring.issue_share(18, 21)

    @pl.when(place > 0)
    def _():
        halo.wait_recv()

    for weight in (0, 1):
        ring.arrive_all(weight)
        loads[inputs + 2 + weight].wait()

    def lift(piece, carry):
        start = pl.multiple_of(piece * own_rows, own_rows)
        rows = normed[pl.ds(start, own_rows + HALO)]
        mixes = []
        for way, weight in enumerate((full_gate, full_up)):
            held = mul(rows, weight[...]).astype(NARROW).astype(WIDE)
            tap = [taps[at][way : way + 1].astype(WIDE) for at in range(3)]
            mixes.append(
                tap[0] * held[HALO - 2 : -2] + tap[1] * held[HALO - 1 : -1] + tap[2] * held[HALO:]
            )
        hidden[pl.ds(start, own_rows)] = (jax.nn.silu(mixes[0]) * mixes[1]).astype(NARROW)

        @pl.when(piece == pieces // 2)
        def _():
            ring.issue_share(19, 21)

        return carry

    lax.fori_loop(0, pieces, lift, 0)
    ring.issue_share(20, 21)

    block = part.shape[2]
    blocks = part.shape[0]
    by_arrival = block == shard
    loads[inputs + 4].wait()
    if not by_arrival:
        ring.issue_to(len(ring.plan))
        ring.arrive_all(2)

    def lanes_of(at):
        if by_arrival:
            odd = lax.rem(at, 2)
            owner = ring.index((2 * odd - 1) * ((at + 1) // 2))
        else:
            owner = at
        return pl.ds(pl.multiple_of(owner * block, block), block)

    def quarter(device):
        return pl.ds(pl.multiple_of(device * own_rows, own_rows), own_rows)

    def near_copy(at, offset):
        return group.copy(
            part.at[at, quarter(group.device(offset, True))],
            near.at[at, offset],
            (near_send, near_recv),
            at * group.half + offset,
            group.device(0, True),
        )

    def far_copy(at, offset):
        return group.copy(
            leaving.at[at, offset - 1],
            far.at[at, offset - 1],
            (far_send, far_recv),
            at * (group.half - 1) + offset - 1,
            group.device(offset, False),
        )

    def close(at, carry):
        if by_arrival:
            for fixed in range(1, blocks):
                hop = (fixed + 1) // 2 - 1

                @pl.when(at == fixed)
                def _():
                    ring.issue_through(2, hop + 1)
                    if hop == around // 2 - 1:
                        ring.arrive_hop(2, hop, 0)
                        ring.arrive_hop(2, hop, 1)
                    else:
                        ring.arrive_hop(2, hop, way_of(fixed))

        @pl.when(at < blocks)
        def _():
            weight = full_down[lanes_of(at)]
            part[at] = mul(hidden[...], weight, ((1,), (1,))).astype(NARROW)
            for offset in list(range(1, group.half)) + [0]:
                near_copy(at, offset).start()

        @pl.when((at >= 1) & (at <= blocks))
        def _():
            done = at - 1
            for offset in range(1, group.half):
                near_copy(done, offset).wait_recv()
                mine = part[done, quarter(group.device(offset, False))].astype(WIDE)
                total = mine + near[done, offset].astype(WIDE)
                leaving[done, offset - 1] = total.astype(NARROW)
                far_copy(done, offset).start()

        @pl.when(at >= LAG)
        def _():
            done = at - LAG
            near_copy(done, 0).wait_recv()
            own = quarter(group.me)
            total = part[done, own].astype(WIDE) + near[done, 0].astype(WIDE)
            for offset in range(1, group.half):
                far_copy(done, offset).wait_recv()
                total = total + far[done, offset - 1].astype(WIDE)
            lanes = lanes_of(done)
            out[:, lanes] = (stream[own, lanes].astype(WIDE) + total).astype(NARROW)

        return carry

    lax.fori_loop(0, blocks + LAG, close, 0)

    ring.finish()
    for step in range(1, around):
        map_copy(step).wait_send()

    @pl.when(place < around - 1)
    def _():
        halo.wait_send()

    def drain_mix(piece, carry):
        mix_spread.finish(piece)
        return carry

    lax.fori_loop(0, pieces, drain_mix, 0)

    def drain_sums(at, carry):
        for offset in range(group.half):
            near_copy(at, offset).wait_send()
        for offset in range(1, group.half):
            far_copy(at, offset).wait_send()
        return carry

    lax.fori_loop(0, blocks, drain_sums, 0)


def way_of(fixed):
    return 1 if fixed % 2 else 0


def layer(*arrays):
    (
        q, k, v, decay, rate, extra, out_gate, residual, out_weight, gate, up, down,
        head_gain, ffn_gain, taps,
    ) = arrays
    tokens, width = q.shape
    own_rows, features = residual.shape
    units = gate.shape[1]
    around, across = lax.axis_size("sp"), lax.axis_size("tp")
    shard = down.shape[0]
    block = shard if shard % 128 == 0 else 256
    blocks = features // block
    half = across // 2
    others = half - 1
    entries = 2 * len(ring_plan(around))
    dma = pltpu.SemaphoreType.DMA

    def two(count):
        return [dma((count,)), dma((count,))]

    def vmem(*shape, dtype=NARROW):
        return pltpu.VMEM(shape, dtype)

    anywhere = pl.BlockSpec(memory_space=pl.ANY)
    near_by = pl.BlockSpec(memory_space=pltpu.VMEM)
    return pl.pallas_call(
        layer_kernel,
        in_specs=[anywhere] * 12 + [near_by] * 3,
        out_specs=near_by,
        out_shape=jax.ShapeDtypeStruct((own_rows, features), NARROW),
        scratch_shapes=[vmem(tokens, width)] * 5
        + [
            vmem(tokens, width, dtype=WIDE),
            vmem(tokens, width),
            vmem(tokens, width, dtype=WIDE),
            vmem(tokens, width, dtype=WIDE),
            vmem(width, 2 * width, dtype=WIDE),
            vmem(around, HEAD_WIDTH, 2 * width),
            vmem(tokens, features),
            vmem(across * width, features),
            vmem(tokens, across * width),
            vmem(HALO + tokens, features),
            vmem(features, units),
            vmem(features, units),
            vmem(features, units),
            vmem(tokens, units),
            vmem(blocks, tokens, block),
            vmem(blocks, half, own_rows, block),
            vmem(blocks, others, own_rows, block),
            vmem(blocks, others, own_rows, block),
            dma((12,)),
        ]
        + two(entries)
        + two(around - 1)
        + [dma, dma]
        + (two(1) + two(others) + two(others)) * 2
        + two(across) + two(across * others) + two(across * others)
        + two(blocks * half)
        + two(blocks * others),
        compiler_params=pltpu.CompilerParams(
            collective_id=1, has_side_effects=True, vmem_limit_bytes=67043328
        ),
        name="layer",
    )(
        q, k, v, decay, rate, extra, out_gate, residual, out_weight, gate, up, down,
        head_gain[None], ffn_gain[None], taps,
    )


def body(
    residual_input_stream,
    receptance,
    key_matrix_all,
    value_matrix_all,
    decay_preactivation,
    learning_rate_preactivation,
    output_gate_all_heads,
    extra_log_decay,
    head_norm_gain,
    output_projection_weight,
    feedforward_norm_gain,
    gate_projection_weight,
    up_projection_weight,
    down_projection_weight,
    convolution_kernel,
):
    return layer(
        receptance,
        key_matrix_all,
        value_matrix_all,
        decay_preactivation,
        learning_rate_preactivation,
        extra_log_decay,
        output_gate_all_heads,
        residual_input_stream,
        output_projection_weight,
        gate_projection_weight,
        up_projection_weight,
        down_projection_weight,
        head_norm_gain,
        feedforward_norm_gain,
        convolution_kernel,
    )


def solution(mesh):
    in_specs = (
        P(("sp", "tp"), None),
        P("sp", "tp"),
        P("sp", "tp"),
        P("sp", "tp"),
        P("sp", "tp"),
        P("sp", "tp"),
        P("sp", "tp"),
        P("sp", "tp"),
        P("tp"),
        P("tp", None),
        P(),
        P("sp", "tp"),
        P("sp", "tp"),
        P("sp", "tp"),
        P(None, None, "tp"),
    )
    out_specs = P(("sp", "tp"), None)
    return jax.shard_map(
        body, mesh=mesh, in_specs=in_specs, out_specs=out_specs, check_vma=False
    )
```

```python
import functools

import jax
import jax.numpy as jnp
from jax import lax
from jax.experimental import pallas as pl
from jax.experimental.pallas import tpu as pltpu
from jax.sharding import PartitionSpec as P

HEAD_WIDTH = 64
BLOCK = 64
PER_STEP = 4
HALO = 16
LAG = 3
LATER = 2
MESH = pl.DeviceIdType.MESH
WIDE = jnp.float32
NARROW = jnp.bfloat16


def mul(a, b, dims=((1,), (0,))):
    return lax.dot_general(
        a.astype(NARROW), b.astype(NARROW), (dims, ((), ())), preferred_element_type=WIDE
    )


def parts_of(a, count):
    found = []
    for _ in range(count):
        piece = a.astype(NARROW)
        found.append(piece)
        a = a - piece.astype(WIDE)
    return found


def fine_left(a, b, count, dims=((1,), (0,))):
    return sum(mul(piece, b, dims) for piece in parts_of(a, count))


def fine_right(a, b, count, dims=((1,), (0,))):
    return sum(mul(a, piece, dims) for piece in parts_of(b, count))


def head_mask(width):
    rows = lax.broadcasted_iota(jnp.int32, (width, width), 0) // HEAD_WIDTH
    lanes = lax.broadcasted_iota(jnp.int32, (width, width), 1) // HEAD_WIDTH
    return jnp.where(rows == lanes, 1.0, 0.0)


def stacked(a, mask):
    a = a.astype(NARROW)
    return jnp.concatenate([a] * (mask.shape[0] // a.shape[0]), axis=0) * mask


def fine_product(a, b, mask):
    a_high, a_low = parts_of(a, 2)
    b_high, b_low = (stacked(piece, mask) for piece in parts_of(b, 2))
    return mul(a_high, b_high) + mul(a_low, b_high) + mul(a_high, b_low)


def collapsed(a):
    heads = a.shape[0] // HEAD_WIDTH
    return sum(a[h * HEAD_WIDTH : (h + 1) * HEAD_WIDTH] for h in range(heads))


def recurrence(refs, local_ref, reach_ref, state, before_step):
    q_ref, k_ref, v_ref, decay_ref, rate_ref, extra_ref = refs
    tokens, width = q_ref.shape
    mask_wide = head_mask(width)
    mask = mask_wide.astype(NARROW)
    last = ((1,), (1,))
    first = ((0,), (0,))

    rows = lax.broadcasted_iota(jnp.int32, (width, width), 0)
    lanes = lax.broadcasted_iota(jnp.int32, (width, width), 1)
    state[:, :width] = jnp.zeros((width, width), WIDE)
    state[:, width:] = jnp.where(rows == lanes, 1.0, 0.0)

    def one(index, carry):
        before_step(index)
        token = lax.broadcasted_iota(jnp.int32, (BLOCK, width), 0)
        other = lax.broadcasted_iota(jnp.int32, (BLOCK, width), 1) % BLOCK
        strict = token > other
        within = token >= other
        eye = jnp.where(token == other, 1.0, 0.0)
        lower = jnp.where(
            lax.broadcasted_iota(jnp.int32, (BLOCK, BLOCK), 0)
            >= lax.broadcasted_iota(jnp.int32, (BLOCK, BLOCK), 1),
            1.0,
            0.0,
        ).astype(NARROW)
        ones = jnp.ones((BLOCK, width), NARROW)

        def window(part):
            return pl.ds(pl.multiple_of((index * PER_STEP + part) * BLOCK, BLOCK), BLOCK)

        prepared = []
        for part in range(PER_STEP):
            at = window(part)
            q = q_ref[at].astype(WIDE)
            k = k_ref[at].astype(WIDE)
            v = stacked(v_ref[at], mask)
            log_decay = (
                -jnp.exp(-0.5) * jax.nn.sigmoid(decay_ref[at].astype(WIDE)) + extra_ref[at]
            )
            rates = jax.nn.sigmoid(rate_ref[at].astype(WIDE))
            normed = k * lax.rsqrt(fine_left(k * k, mask, 2) + 1e-06)
            removal = normed * rates
            cum = fine_right(lower, log_decay, 3)
            previous = cum - log_decay
            middle = cum[BLOCK // 2 : BLOCK // 2 + 1]
            end = cum[BLOCK - 1 : BLOCK]
            back = jnp.exp(middle - cum)
            left = jnp.concatenate(
                [normed * jnp.exp(previous - middle), q * jnp.exp(cum - middle)], axis=0
            )
            by_key = mul(left, stacked(k * back, mask), last)
            by_removal = mul(left, stacked(removal * back, mask), last)
            key_rate = jnp.where(strict, by_key[:BLOCK], 0.0)
            removal_rate = jnp.where(strict, by_removal[:BLOCK], 0.0)
            key_out = jnp.where(within, by_key[BLOCK:], 0.0)
            removal_out = jnp.where(within, by_removal[BLOCK:], 0.0)
            inverse = eye
            size = 1
            while size < BLOCK:
                pair = (token // (2 * size) == other // (2 * size)) & (
                    token // size != other // size
                )
                piece = jnp.where(pair, removal_rate, 0.0)
                if size == 1:
                    inverse = inverse - piece
                else:
                    inverse = inverse - fine_product(
                        fine_product(inverse, piece, mask), inverse, mask
                    )
                size *= 2
            from_state = mul(inverse, stacked(normed * jnp.exp(previous), mask))
            keyed = mul(jnp.concatenate([key_rate, key_out], axis=0), v)
            offset = mul(inverse, stacked(keyed[:BLOCK], mask))
            reach = q * jnp.exp(cum) - mul(removal_out, stacked(from_state, mask))
            local = keyed[BLOCK:] - mul(removal_out, stacked(offset, mask))
            to_end = jnp.exp(end - cum)
            span = jnp.exp(fine_left(log_decay, ones, 3, first))
            prepared.append((from_state, offset, reach, local, k * to_end, removal * to_end, span))

        for part in range(PER_STEP):
            at = window(part)
            from_state, offset, reach, local, key_end, removal_end, span = prepared[part]
            now = state[...]
            both = mul(jnp.concatenate([from_state, reach], axis=0), now)
            correction = both[:BLOCK, :width] + offset
            local_ref[at] = local + both[BLOCK:, :width]
            reach_ref[at] = both[BLOCK:, width:]
            kept_value = mul(
                jnp.concatenate([key_end, -removal_end], axis=0),
                jnp.concatenate([v_ref[at].astype(WIDE), correction], axis=0),
                first,
            )
            kept_map = mul(-removal_end, both[:BLOCK, width:], first)
            state[:, :width] = now[:, :width] * span + kept_value * mask_wide
            state[:, width:] = now[:, width:] * span + kept_map * mask_wide
        return carry

    lax.fori_loop(0, tokens // (BLOCK * PER_STEP), one, 0)


def halves_of(units):
    window = -(-units // 256) * 128
    return window, units - window


class Lines:
    def __init__(self, axis, shards, gathered, over_sems, across_sems):
        self.axis, self.shards, self.gathered = axis, shards, gathered
        self.over_sems, self.across_sems = over_sems, across_sems
        me = lax.axis_index(axis)
        self.outer = lax.axis_size(axis) // 2
        self.line = me // 2
        self.side = lax.rem(me, 2)
        self.pair = self.line + 1 - 2 * lax.rem(self.line, 2)
        self.shard = shards[0].shape[0]
        self.step = self.shard // 2
        self.window, self.shift = halves_of(shards[0].shape[1])

    def share(self, line):
        return lax.rem(line + line // 2, 2)

    def lanes(self, line):
        return pl.ds(pl.multiple_of(self.share(line) * self.shift, 128), self.window)

    def line_at(self, offset):
        return lax.rem(self.line + offset + self.outer, self.outer)

    def source(self, entry, line):
        weight, half = divmod(entry, 2)
        return self.shards[weight].at[pl.ds(half * self.step, self.step), self.lanes(line)]

    def target(self, entry, line, side):
        weight, half = divmod(entry, 2)
        start = (line * 2 + side) * self.shard + half * self.step
        return self.gathered[weight].at[pl.ds(pl.multiple_of(start, self.step), self.step)]

    def copy(self, source, target, sems, slot, device):
        return pltpu.make_async_remote_copy(
            src_ref=source,
            dst_ref=target,
            send_sem=sems[0].at[slot],
            recv_sem=sems[1].at[slot],
            device_id={self.axis: device},
            device_id_type=MESH,
        )

    def over(self, entry, offset):
        line = self.line_at(offset)
        return self.copy(
            self.source(entry, line),
            self.target(entry, self.line, self.side),
            self.over_sems,
            entry * (self.outer - 1) + offset - 1,
            line * 2 + self.side,
        )

    def across(self, entry, offset):
        target = self.target(entry, self.line_at(-offset), self.side)
        return self.copy(
            self.source(entry, self.line) if offset == 0 else target,
            target,
            self.across_sems,
            entry * self.outer + offset,
            self.line * 2 + 1 - self.side,
        )

    def send(self, entry):
        for offset in range(1, self.outer):
            self.over(entry, offset).start()

    def own(self, entry):
        self.across(entry, 0).start()

    def pump(self, entry):
        for offset in range(1, self.outer):
            self.over(entry, offset).wait_recv()
            self.across(entry, offset).start()

    def arrive(self, entry):
        for offset in range(self.outer):
            self.across(entry, offset).wait_recv()

    def finish(self):
        for entry in range(6):
            for offset in range(1, self.outer):
                self.over(entry, offset).wait_send()
            for offset in range(self.outer):
                self.across(entry, offset).wait_send()


class Group:
    def __init__(self, axis):
        self.axis = axis
        self.count = lax.axis_size(axis)
        self.me = lax.axis_index(axis)
        self.half = self.count // 2

    def device(self, offset, sibling):
        side = lax.rem(self.me, 2)
        group = lax.rem(self.me // 2 + offset + self.half, self.half)
        return 2 * group + (1 - side if sibling else side)

    def turn(self, step, ahead):
        side = lax.rem(self.me, 2)
        group = lax.rem(self.me // 2 + ahead + step // 2, self.half)
        return 2 * group + lax.rem(side + step, 2)

    def copy(self, source, target, sems, slot, device):
        return pltpu.make_async_remote_copy(
            src_ref=source,
            dst_ref=target,
            send_sem=sems[0].at[slot],
            recv_sem=sems[1].at[slot],
            device_id={self.axis: device},
            device_id_type=MESH,
        )


class Spread:
    def __init__(self, group, source, block, side_sems, far_sems, pass_sems):
        self.group, self.source, self.block = group, source, block
        self.side_sems, self.far_sems, self.pass_sems = side_sems, far_sems, pass_sems
        self.others = range(1, group.half)

    def slot(self, piece, offset):
        return piece * (self.group.half - 1) + offset - 1

    def side(self, piece):
        group = self.group
        return group.copy(
            self.source(piece), self.block(group.me, piece), self.side_sems, piece,
            group.device(0, True),
        )

    def far(self, piece, offset):
        group = self.group
        return group.copy(
            self.source(piece), self.block(group.me, piece), self.far_sems,
            self.slot(piece, offset), group.device(offset, False),
        )

    def onward(self, piece, offset):
        group = self.group
        block = self.block(group.device(-offset, False), piece)
        return group.copy(
            block, block, self.pass_sems, self.slot(piece, offset), group.device(0, True)
        )

    def start(self, piece):
        for offset in self.others:
            self.far(piece, offset).start()
        self.side(piece).start()

    def hand_on(self, piece):
        for offset in self.others:
            self.far(piece, offset).wait_recv()
            self.onward(piece, offset).start()

    def arrive(self, piece):
        self.side(piece).wait_recv()
        for offset in self.others:
            self.onward(piece, offset).wait_recv()

    def finish(self, piece):
        self.side(piece).wait_send()
        for offset in self.others:
            self.far(piece, offset).wait_send()
            self.onward(piece, offset).wait_send()


def layer_kernel(
    q_in, k_in, v_in, decay_in, rate_in, extra_in, out_gate_in, residual_in, out_weight_in,
    gate_in, up_in, down_in, head_gain, ffn_gain, taps,
    out,
    q, k, v, decay, rate, extra, out_gate, local, reach, state, maps,
    stream, out_weight, mixed, normed, others_normed, full_gate, full_up, full_down, hidden,
    part, near, leaving, far, kept_sum, lent, returned, result,
    load_sem, out_sem, over_send, over_recv, across_send, across_recv,
    map_over_send, map_over_recv, map_across_send, map_across_recv,
    halo_send, halo_recv, lend_send, lend_recv,
    rows_side_send, rows_side_recv, rows_far_send, rows_far_recv, rows_pass_send, rows_pass_recv,
    wide_side_send, wide_side_recv, wide_far_send, wide_far_recv, wide_pass_send, wide_pass_recv,
    mix_side_send, mix_side_recv, mix_far_send, mix_far_recv, mix_pass_send, mix_pass_recv,
    norm_side_send, norm_side_recv, norm_far_send, norm_far_recv, norm_pass_send, norm_pass_recv,
    near_send, near_recv, far_send, far_recv, return_send, return_recv,
):
    tokens, width = q.shape
    features = stream.shape[1]
    group = Group("tp")
    around = lax.axis_size("sp")
    place = lax.axis_index("sp")
    own_rows = tokens // group.count
    lines = Lines(
        "sp", (gate_in, up_in, down_in), (full_gate, full_up, full_down),
        (over_send, over_recv), (across_send, across_recv),
    )
    outer, line, side = lines.outer, lines.line, lines.side
    partner = lines.pair * 2 + side
    shard = down_in.shape[0]

    def owned(ref, index, rows):
        return ref.at[pl.ds(pl.multiple_of(index * rows, rows), rows)]

    def at_sp(source, target, sems, slot, device):
        return lines.copy(source, target, sems, slot, device)

    pairs = list(
        zip(
            (q_in, k_in, v_in, decay_in, rate_in, extra_in, out_gate_in),
            (q, k, v, decay, rate, extra, out_gate),
        )
    )
    inputs = len(pairs)
    pairs += [
        (residual_in, owned(stream, group.me, own_rows)),
        (out_weight_in, owned(out_weight, group.me, width)),
    ]
    pairs += [
        (whole.at[:, lines.lanes(line)], owned(full, place, shard))
        for whole, full in zip(lines.shards, lines.gathered)
    ]
    loads = [
        pltpu.make_async_copy(source, target, load_sem.at[at])
        for at, (source, target) in enumerate(pairs)
    ]
    for load in loads[:inputs]:
        load.start()

    barrier = pltpu.get_barrier_semaphore()
    for axis, count, me in (("sp", around, place), ("tp", group.count, group.me)):
        for step in range(1, count):
            pl.semaphore_signal(
                barrier, inc=1, device_id={axis: lax.rem(me + step, count)}, device_id_type=MESH
            )
    pl.semaphore_wait(barrier, around + group.count - 2)

    lines.send(0)
    lines.send(1)
    for entry in range(4):
        lines.own(entry)
    rows_spread = Spread(
        group,
        lambda piece: residual_in,
        lambda index, piece: owned(stream, index, own_rows),
        (rows_side_send, rows_side_recv),
        (rows_far_send, rows_far_recv),
        (rows_pass_send, rows_pass_recv),
    )
    wide_spread = Spread(
        group,
        lambda piece: out_weight_in,
        lambda index, piece: owned(out_weight, index, width),
        (wide_side_send, wide_side_recv),
        (wide_far_send, wide_far_recv),
        (wide_pass_send, wide_pass_recv),
    )
    rows_spread.start(0)
    wide_spread.start(0)
    for load in loads[inputs:]:
        load.start()
    for load in loads[:inputs]:
        load.wait()

    steps = tokens // (BLOCK * PER_STEP)

    def before_step(index):
        @pl.when(index == steps // 2)
        def _():
            lines.pump(0)
            lines.own(4)
            lines.own(5)
            lines.send(2)

        @pl.when(index == steps - 1)
        def _():
            lines.pump(1)

    recurrence((q, k, v, decay, rate, extra), local, reach, state, before_step)

    def map_over(offset):
        return at_sp(
            maps.at[place], maps.at[place], (map_over_send, map_over_recv), offset - 1,
            lax.rem(line + offset, outer) * 2 + side,
        )

    def map_across(offset):
        held = maps.at[lines.line_at(-offset) * 2 + side]
        return at_sp(
            held, held, (map_across_send, map_across_recv), offset, line * 2 + 1 - side
        )

    maps[place] = collapsed(state[...]).astype(NARROW)
    for offset in range(1, outer):

        @pl.when(line + offset < outer)
        def _():
            map_over(offset).start()

    map_across(0).start()
    lines.send(3)
    rows_spread.hand_on(0)
    wide_spread.hand_on(0)
    for offset in range(1, outer):

        @pl.when(line >= offset)
        def _():
            map_over(offset).wait_recv()
            map_across(offset).start()

    lines.pump(2)
    map_across(0).wait_recv()
    for offset in range(1, outer):

        @pl.when(line >= offset)
        def _():
            map_across(offset).wait_recv()

    mask = head_mask(width).astype(NARROW)

    def enter(step, entering):
        found = maps[step]
        high, low = parts_of(entering, 2)
        after = (
            found[:, :width].astype(WIDE)
            + mul(found[:, width:], stacked(high, mask))
            + mul(found[:, width:], stacked(low, mask))
        )
        return after

    entering = lax.fori_loop(0, place, enter, jnp.zeros((HEAD_WIDTH, width), WIDE))
    state[:, :width] = stacked(entering, mask).astype(WIDE)

    pieces = group.count
    own_lanes = pl.ds(pl.multiple_of(group.me * width, width), width)

    def rows_at(piece):
        return pl.ds(pl.multiple_of(piece * own_rows, own_rows), own_rows)

    def mixed_block(index, piece):
        return mixed.at[rows_at(piece), pl.ds(pl.multiple_of(index * width, width), width)]

    mix_spread = Spread(
        group,
        lambda piece: mixed_block(group.me, piece),
        mixed_block,
        (mix_side_send, mix_side_recv),
        (mix_far_send, mix_far_recv),
        (mix_pass_send, mix_pass_recv),
    )

    def mix(step, carry):
        piece = group.turn(step, 1)
        rows = rows_at(piece)
        readout = local[rows] + mul(reach[rows], state[:, :width])
        centered = readout - fine_left(readout, mask, 2) * (1.0 / HEAD_WIDTH)
        variance = fine_left(centered * centered, mask, 2) * (1.0 / HEAD_WIDTH)
        value = (
            centered
            * lax.rsqrt(variance + 0.00064)
            * head_gain[...]
            * out_gate[rows].astype(WIDE)
        )
        mixed[rows, own_lanes] = value.astype(NARROW)
        mix_spread.start(piece)
        return carry

    lax.fori_loop(0, pieces, mix, 0)
    lines.send(4)
    rows_spread.arrive(0)
    wide_spread.arrive(0)
    rows_spread.finish(0)
    wide_spread.finish(0)
    loads[inputs].wait()
    loads[inputs + 1].wait()

    small = own_rows // pieces

    def lend_rows(index, piece):
        start = HALO + index * own_rows + piece * small
        return pl.ds(pl.multiple_of(start, HALO), small)

    def lend(piece):
        rows = lend_rows(group.me, piece)
        return at_sp(
            normed.at[rows], others_normed.at[rows], (lend_send, lend_recv), piece, partner
        )

    norm_spread = Spread(
        group,
        lambda piece: others_normed.at[lend_rows(group.me, piece)],
        lambda index, piece: others_normed.at[lend_rows(index, piece)],
        (norm_side_send, norm_side_recv),
        (norm_far_send, norm_far_recv),
        (norm_pass_send, norm_pass_recv),
    )

    def settle(step, carry):
        @pl.when(step < pieces)
        def _():
            mix_spread.hand_on(group.turn(step, 0))

        @pl.when(step > 0)
        def _():
            done = group.turn(step - 1, 0)
            mix_spread.arrive(done)
            rows = rows_at(done)
            total = mul(mixed[rows], out_weight[...])
            kept = (stream[rows].astype(WIDE) + total).astype(NARROW)
            stream[rows] = kept
            kept = kept.astype(WIDE)
            scale = lax.rsqrt(jnp.mean(kept * kept, axis=-1, keepdims=True) + 1e-06)
            after = pl.ds(pl.multiple_of(HALO + done * own_rows, HALO), own_rows)
            normed[after] = (kept * scale * ffn_gain[...]).astype(NARROW)

        @pl.when(step == 1)
        def _():
            for piece in range(pieces):
                lend(piece).start()

        return carry

    lax.fori_loop(0, pieces + 1, settle, 0)

    following = place + 1
    following_pair = (
        following // 2 + 1 - 2 * lax.rem(following // 2, 2)
    ) * 2 + lax.rem(following, 2)
    tail, head = pl.ds(tokens, HALO), pl.ds(0, HALO)
    halo_sems = (halo_send, halo_recv)
    halo = at_sp(normed.at[tail], normed.at[head], halo_sems, 0, lax.rem(following, around))
    halo_lent = at_sp(
        normed.at[tail], others_normed.at[head], halo_sems, 1, lax.rem(following_pair, around)
    )

    @pl.when(place < around - 1)
    def _():
        halo.start()
        halo_lent.start()

    @pl.when(place == 0)
    def _():
        normed[:HALO] = jnp.zeros((HALO, features), NARROW)

    @pl.when(partner == 0)
    def _():
        others_normed[:HALO] = jnp.zeros((HALO, features), NARROW)

    lines.send(5)
    lines.pump(3)

    @pl.when(place > 0)
    def _():
        halo.wait_recv()

    for entry in range(4):
        lines.arrive(entry)
    loads[inputs + 2].wait()
    loads[inputs + 3].wait()
    spare = lines.window - lines.shift

    def lift(source, base, piece):
        start = pl.multiple_of(piece * own_rows, own_rows)
        rows = source[pl.ds(start, own_rows + HALO)]
        mixes = []
        for way, weight in enumerate((full_gate, full_up)):
            held = mul(rows, weight[...]).astype(NARROW).astype(WIDE)
            tap = [taps[at, pl.ds(way, 1), lines.lanes(line)].astype(WIDE) for at in range(3)]
            mixes.append(
                tap[0] * held[HALO - 2 : -2] + tap[1] * held[HALO - 1 : -1] + tap[2] * held[HALO:]
            )
        to = pl.ds(pl.multiple_of(base + start, own_rows), own_rows)
        hidden[to] = (jax.nn.silu(mixes[0]) * mixes[1]).astype(NARROW)
        if spare:

            @pl.when(lines.share(line) == 1)
            def _():
                hidden[to, :spare] = jnp.zeros((own_rows, spare), NARROW)

    def lift_own(piece, carry):
        lend(piece).wait_recv()
        norm_spread.start(piece)

        @pl.when(piece > 0)
        def _():
            norm_spread.hand_on(piece - 1)

        lift(normed, 0, piece)
        return carry

    lax.fori_loop(0, pieces, lift_own, 0)
    norm_spread.hand_on(pieces - 1)
    lines.pump(4)

    block = part.shape[2]
    slots = part.shape[0]
    spans = slots // 2
    units = 2 * slots
    by_arrival = lines.step == block // 2 and spans == outer
    lines.arrive(4)
    loads[inputs + 4].wait()

    def last_weights():
        lines.pump(5)
        lines.arrive(5)

    if not by_arrival:
        last_weights()

    def feature_block(unit):
        return unit // (2 * spans) * spans + lax.rem(unit, spans)

    def whose(unit):
        return lax.rem(unit // spans, 2)

    def starts_of(index):
        if by_arrival:
            first = lax.rem(index, spans) * 2 * shard + index // spans * lines.step
            found = (first, first + shard)
        else:
            found = (index * block, index * block + block // 2)
        return [pl.ds(pl.multiple_of(start, block // 2), block // 2) for start in found]

    def near_copy(unit, offset):
        return group.copy(
            part.at[lax.rem(unit, slots), rows_at(group.device(offset, True))],
            near.at[unit, offset],
            (near_send, near_recv),
            unit * group.half + offset,
            group.device(0, True),
        )

    def far_copy(unit, offset):
        return group.copy(
            leaving.at[unit, offset - 1],
            far.at[unit, offset - 1],
            (far_send, far_recv),
            unit * (group.half - 1) + offset - 1,
            group.device(offset, False),
        )

    def give_back(index):
        return at_sp(
            lent.at[index], returned.at[index], (return_send, return_recv), index, partner
        )

    def out_copy(index, way):
        lanes = starts_of(index)[way]
        return pltpu.make_async_copy(
            result.at[:, lanes], out.at[:, lanes], out_sem.at[2 * index + way]
        )

    own = rows_at(group.me)

    def close(step, carry):
        pause = spans
        unit = jnp.where(step > pause, step - 1, step)

        @pl.when((step == 2 * spans + 1) & by_arrival)
        def _():
            if by_arrival:
                last_weights()

        @pl.when((step != pause) & (unit < units))
        def _():
            @pl.when(unit >= slots)
            def _():
                for offset in range(group.half):
                    near_copy(unit - slots, offset).wait_send()

            weight = jnp.concatenate(
                [full_down[rows] for rows in starts_of(feature_block(unit))], axis=0
            )
            rows = hidden[pl.ds(pl.multiple_of(whose(unit) * tokens, tokens), tokens)]
            part[lax.rem(unit, slots)] = mul(rows, weight, ((1,), (1,))).astype(NARROW)
            for offset in list(range(1, group.half)) + [0]:
                near_copy(unit, offset).start()

        ready = jnp.where(step > pause, step - 2, step - 1)

        @pl.when((step >= 1) & (step != pause + 1) & (ready < units))
        def _():
            for offset in range(1, group.half):
                near_copy(ready, offset).wait_recv()
                mine = part[lax.rem(ready, slots), rows_at(group.device(offset, False))]
                total = mine.astype(WIDE) + near[ready, offset].astype(WIDE)
                leaving[ready, offset - 1] = total.astype(NARROW)
                far_copy(ready, offset).start()

        @pl.when(step == pause)
        def _():
            @pl.when(partner > 0)
            def _():
                halo_lent.wait_recv()

            def lift_lent(piece, carry):
                lift(others_normed, tokens, piece)
                return carry

            for piece in range(pieces):
                norm_spread.arrive(piece)
            lax.fori_loop(0, pieces, lift_lent, 0)

        done = step - 1 - LAG

        @pl.when((done >= 0) & (done < units))
        def _():
            near_copy(done, 0).wait_recv()
            total = part[lax.rem(done, slots), own].astype(WIDE) + near[done, 0].astype(WIDE)
            for offset in range(1, group.half):
                far_copy(done, offset).wait_recv()
                total = total + far[done, offset - 1].astype(WIDE)
            index = feature_block(done)

            @pl.when(whose(done) == 0)
            def _():
                kept = [stream[own, lanes].astype(WIDE) for lanes in starts_of(index)]
                kept_sum[index] = total + jnp.concatenate(kept, axis=1)

            @pl.when(whose(done) == 1)
            def _():
                lent[index] = total.astype(NARROW)
                give_back(index).start()

        last = done - LATER

        @pl.when((last >= 0) & (last < units) & (whose(jnp.maximum(last, 0)) == 1))
        def _():
            index = feature_block(last)
            give_back(index).wait_recv()
            total = (kept_sum[index] + returned[index].astype(WIDE)).astype(NARROW)
            for way, lanes in enumerate(starts_of(index)):
                result[:, lanes] = total[:, way * (block // 2) : (way + 1) * (block // 2)]
                out_copy(index, way).start()

        return carry

    lax.fori_loop(0, units + 1 + LAG + LATER, close, 0)

    lines.finish()
    map_across(0).wait_send()
    for offset in range(1, outer):

        @pl.when(line + offset < outer)
        def _():
            map_over(offset).wait_send()

        @pl.when(line >= offset)
        def _():
            map_across(offset).wait_send()

    @pl.when(place < around - 1)
    def _():
        halo.wait_send()
        halo_lent.wait_send()

    for piece in range(pieces):
        mix_spread.finish(piece)
        norm_spread.finish(piece)
        lend(piece).wait_send()

    def drain(unit, carry):
        @pl.when(unit >= units - slots)
        def _():
            for offset in range(group.half):
                near_copy(unit, offset).wait_send()

        for offset in range(1, group.half):
            far_copy(unit, offset).wait_send()

        @pl.when(unit < slots)
        def _():
            give_back(unit).wait_send()
            for way in (0, 1):
                out_copy(unit, way).wait()

        return carry

    lax.fori_loop(0, units, drain, 0)


def layer(*arrays):
    (
        q, k, v, decay, rate, extra, out_gate, residual, out_weight, gate, up, down,
        head_gain, ffn_gain, taps,
    ) = arrays
    tokens, width = q.shape
    own_rows, features = residual.shape
    window, _ = halves_of(gate.shape[1])
    around, across = lax.axis_size("sp"), lax.axis_size("tp")
    outer = around // 2
    block = 256
    slots = features // block
    work = 2 * slots
    half = across // 2
    others = half - 1
    dma = pltpu.SemaphoreType.DMA

    def two(count):
        return [dma((count,)), dma((count,))]

    def vmem(*shape, dtype=NARROW):
        return pltpu.VMEM(shape, dtype)

    anywhere = pl.BlockSpec(memory_space=pl.ANY)
    near_by = pl.BlockSpec(memory_space=pltpu.VMEM)
    return pl.pallas_call(
        layer_kernel,
        in_specs=[anywhere] * 12 + [near_by] * 3,
        out_specs=anywhere,
        out_shape=jax.ShapeDtypeStruct((own_rows, features), NARROW),
        scratch_shapes=[vmem(tokens, width)] * 5
        + [
            vmem(tokens, width, dtype=WIDE),
            vmem(tokens, width),
            vmem(tokens, width, dtype=WIDE),
            vmem(tokens, width, dtype=WIDE),
            vmem(width, 2 * width, dtype=WIDE),
            vmem(around, HEAD_WIDTH, 2 * width),
            vmem(tokens, features),
            vmem(across * width, features),
            vmem(tokens, across * width),
            vmem(HALO + tokens, features),
            vmem(HALO + tokens, features),
            vmem(features, window),
            vmem(features, window),
            vmem(features, window),
            vmem(2 * tokens, window),
            vmem(slots, tokens, block),
            vmem(work, half, own_rows, block),
            vmem(work, others, own_rows, block),
            vmem(work, others, own_rows, block),
            vmem(slots, own_rows, block, dtype=WIDE),
            vmem(slots, own_rows, block),
            vmem(slots, own_rows, block),
            vmem(own_rows, features),
            dma((12,)),
            dma((2 * slots,)),
        ]
        + two(6 * (outer - 1))
        + two(6 * outer)
        + two(outer - 1)
        + two(outer)
        + two(2)
        + two(across)
        + (two(1) + two(others) + two(others)) * 2
        + (two(across) + two(across * others) + two(across * others)) * 2
        + two(work * half)
        + two(work * others)
        + two(slots),
        compiler_params=pltpu.CompilerParams(
            collective_id=1, has_side_effects=True, vmem_limit_bytes=67043328
        ),
        name="layer",
    )(
        q, k, v, decay, rate, extra, out_gate, residual, out_weight, gate, up, down,
        head_gain[None], ffn_gain[None], taps,
    )


def body(
    residual_input_stream,
    receptance,
    key_matrix_all,
    value_matrix_all,
    decay_preactivation,
    learning_rate_preactivation,
    output_gate_all_heads,
    extra_log_decay,
    head_norm_gain,
    output_projection_weight,
    feedforward_norm_gain,
    gate_projection_weight,
    up_projection_weight,
    down_projection_weight,
    convolution_kernel,
):
    return layer(
        receptance,
        key_matrix_all,
        value_matrix_all,
        decay_preactivation,
        learning_rate_preactivation,
        extra_log_decay,
        output_gate_all_heads,
        residual_input_stream,
        output_projection_weight,
        gate_projection_weight,
        up_projection_weight,
        down_projection_weight,
        head_norm_gain,
        feedforward_norm_gain,
        convolution_kernel,
    )


def solution(mesh):
    in_specs = (
        P(("sp", "tp"), None),
        P("sp", "tp"),
        P("sp", "tp"),
        P("sp", "tp"),
        P("sp", "tp"),
        P("sp", "tp"),
        P("sp", "tp"),
        P("sp", "tp"),
        P("tp"),
        P("tp", None),
        P(),
        P("sp", "tp"),
        P("sp", "tp"),
        P("sp", "tp"),
        P(None, None, "tp"),
    )
    out_specs = P(("sp", "tp"), None)
    return jax.shard_map(
        body, mesh=mesh, in_specs=in_specs, out_specs=out_specs, check_vma=False
    )
```

```python
import functools

import jax
import jax.numpy as jnp
from jax import lax
from jax.experimental import pallas as pl
from jax.experimental.pallas import tpu as pltpu
from jax.sharding import PartitionSpec as P

HEAD_WIDTH = 64
BLOCK = 64
PER_STEP = 4
HALO = 16
LAG = 3
MESH = pl.DeviceIdType.MESH
WIDE = jnp.float32
NARROW = jnp.bfloat16


def mul(a, b, dims=((1,), (0,))):
    return lax.dot_general(
        a.astype(NARROW), b.astype(NARROW), (dims, ((), ())), preferred_element_type=WIDE
    )


def parts_of(a, count):
    found = []
    for _ in range(count):
        piece = a.astype(NARROW)
        found.append(piece)
        a = a - piece.astype(WIDE)
    return found


def fine_left(a, b, count, dims=((1,), (0,))):
    return sum(mul(piece, b, dims) for piece in parts_of(a, count))


def fine_right(a, b, count, dims=((1,), (0,))):
    return sum(mul(a, piece, dims) for piece in parts_of(b, count))


def head_mask(width):
    rows = lax.broadcasted_iota(jnp.int32, (width, width), 0) // HEAD_WIDTH
    lanes = lax.broadcasted_iota(jnp.int32, (width, width), 1) // HEAD_WIDTH
    return jnp.where(rows == lanes, 1.0, 0.0)


def stacked(a, mask):
    a = a.astype(NARROW)
    return jnp.concatenate([a] * (mask.shape[0] // a.shape[0]), axis=0) * mask


def fine_product(a, b, mask):
    a_high, a_low = parts_of(a, 2)
    b_high, b_low = (stacked(piece, mask) for piece in parts_of(b, 2))
    return mul(a_high, b_high) + mul(a_low, b_high) + mul(a_high, b_low)


def collapsed(a):
    heads = a.shape[0] // HEAD_WIDTH
    return sum(a[h * HEAD_WIDTH : (h + 1) * HEAD_WIDTH] for h in range(heads))


def recurrence(refs, local_ref, reach_ref, state, before_step):
    q_ref, k_ref, v_ref, decay_ref, rate_ref, extra_ref = refs
    tokens, width = q_ref.shape
    mask_wide = head_mask(width)
    mask = mask_wide.astype(NARROW)
    last = ((1,), (1,))
    first = ((0,), (0,))

    rows = lax.broadcasted_iota(jnp.int32, (width, width), 0)
    lanes = lax.broadcasted_iota(jnp.int32, (width, width), 1)
    state[:, :width] = jnp.zeros((width, width), WIDE)
    state[:, width:] = jnp.where(rows == lanes, 1.0, 0.0)

    def one(index, carry):
        before_step(index)
        token = lax.broadcasted_iota(jnp.int32, (BLOCK, width), 0)
        other = lax.broadcasted_iota(jnp.int32, (BLOCK, width), 1) % BLOCK
        strict = token > other
        within = token >= other
        eye = jnp.where(token == other, 1.0, 0.0)
        lower = jnp.where(
            lax.broadcasted_iota(jnp.int32, (BLOCK, BLOCK), 0)
            >= lax.broadcasted_iota(jnp.int32, (BLOCK, BLOCK), 1),
            1.0,
            0.0,
        ).astype(NARROW)
        ones = jnp.ones((BLOCK, width), NARROW)

        def window(part):
            return pl.ds(pl.multiple_of((index * PER_STEP + part) * BLOCK, BLOCK), BLOCK)

        prepared = []
        for part in range(PER_STEP):
            at = window(part)
            q = q_ref[at].astype(WIDE)
            k = k_ref[at].astype(WIDE)
            v = stacked(v_ref[at], mask)
            log_decay = (
                -jnp.exp(-0.5) * jax.nn.sigmoid(decay_ref[at].astype(WIDE)) + extra_ref[at]
            )
            rates = jax.nn.sigmoid(rate_ref[at].astype(WIDE))
            normed = k * lax.rsqrt(fine_left(k * k, mask, 2) + 1e-06)
            removal = normed * rates
            cum = fine_right(lower, log_decay, 3)
            previous = cum - log_decay
            middle = cum[BLOCK // 2 : BLOCK // 2 + 1]
            end = cum[BLOCK - 1 : BLOCK]
            back = jnp.exp(middle - cum)
            left = jnp.concatenate(
                [normed * jnp.exp(previous - middle), q * jnp.exp(cum - middle)], axis=0
            )
            by_key = mul(left, stacked(k * back, mask), last)
            by_removal = mul(left, stacked(removal * back, mask), last)
            key_rate = jnp.where(strict, by_key[:BLOCK], 0.0)
            removal_rate = jnp.where(strict, by_removal[:BLOCK], 0.0)
            key_out = jnp.where(within, by_key[BLOCK:], 0.0)
            removal_out = jnp.where(within, by_removal[BLOCK:], 0.0)
            inverse = eye
            size = 1
            while size < BLOCK:
                pair = (token // (2 * size) == other // (2 * size)) & (
                    token // size != other // size
                )
                piece = jnp.where(pair, removal_rate, 0.0)
                if size == 1:
                    inverse = inverse - piece
                else:
                    inverse = inverse - fine_product(
                        fine_product(inverse, piece, mask), inverse, mask
                    )
                size *= 2
            from_state = mul(inverse, stacked(normed * jnp.exp(previous), mask))
            keyed = mul(jnp.concatenate([key_rate, key_out], axis=0), v)
            offset = mul(inverse, stacked(keyed[:BLOCK], mask))
            reach = q * jnp.exp(cum) - mul(removal_out, stacked(from_state, mask))
            local = keyed[BLOCK:] - mul(removal_out, stacked(offset, mask))
            to_end = jnp.exp(end - cum)
            span = jnp.exp(fine_left(log_decay, ones, 3, first))
            prepared.append((from_state, offset, reach, local, k * to_end, removal * to_end, span))

        for part in range(PER_STEP):
            at = window(part)
            from_state, offset, reach, local, key_end, removal_end, span = prepared[part]
            now = state[...]
            both = mul(jnp.concatenate([from_state, reach], axis=0), now)
            correction = both[:BLOCK, :width] + offset
            local_ref[at] = local + both[BLOCK:, :width]
            reach_ref[at] = both[BLOCK:, width:]
            kept_value = mul(
                jnp.concatenate([key_end, -removal_end], axis=0),
                jnp.concatenate([v_ref[at].astype(WIDE), correction], axis=0),
                first,
            )
            kept_map = mul(-removal_end, both[:BLOCK, width:], first)
            state[:, :width] = now[:, :width] * span + kept_value * mask_wide
            state[:, width:] = now[:, width:] * span + kept_map * mask_wide
        return carry

    lax.fori_loop(0, tokens // (BLOCK * PER_STEP), one, 0)


def ring_plan(count):
    hops = count // 2

    def entries(weight, hop):
        if hop < hops - 1:
            return [(weight, 0, hop), (weight, 1, hop)]
        return [(weight, None, hop)]

    plan = []
    for weight in range(3):
        plan += entries(weight, 0)
    for hop in range(1, hops):
        plan += entries(0, hop) + entries(1, hop)
    for hop in range(1, hops):
        plan += entries(2, hop)
    return plan


class Ring:
    def __init__(self, axis, shards, gathered, sems):
        self.axis, self.shards, self.gathered, self.sems = axis, shards, gathered, sems
        self.count = lax.axis_size(axis)
        me = lax.axis_index(axis)
        odd = lax.rem(me, 2)
        self.place = (1 - odd) * (me // 2) + odd * (self.count - 1 - me // 2)
        self.plan = ring_plan(self.count)
        self.number = {}
        for at, (weight, half, hop) in enumerate(self.plan):
            for way in (0, 1):
                self.number[weight, way if half is None else half, hop, way] = at
        self.issued = 0
        self.waited = set()

    def index(self, offset):
        at = lax.rem(self.place + offset + 2 * self.count, self.count)
        upper = at // (self.count // 2)
        return (1 - upper) * 2 * at + upper * (2 * (self.count - 1 - at) + 1)

    def block(self, weight, half, offset):
        rows = self.shards[weight].shape[0]
        start = self.index(offset) * rows + half * (rows // 2)
        return self.gathered[weight].at[pl.ds(pl.multiple_of(start, rows // 2), rows // 2)]

    def copy(self, at, way):
        weight, half, hop = self.plan[at]
        half = way if half is None else half
        rows = self.shards[weight].shape[0] // 2
        back = -hop if way == 0 else hop
        target = self.block(weight, half, back)
        source = self.shards[weight].at[pl.ds(half * rows, rows)] if hop == 0 else target
        slot = 2 * at + way
        return pltpu.make_async_remote_copy(
            src_ref=source,
            dst_ref=target,
            send_sem=self.sems[0].at[slot],
            recv_sem=self.sems[1].at[slot],
            device_id={self.axis: self.index(1 if way == 0 else -1)},
            device_id_type=MESH,
        )

    def arrive(self, weight, half, hop, way):
        at = self.number[weight, half, hop, way]
        if (at, way) not in self.waited:
            self.waited.add((at, way))
            self.copy(at, way).wait_recv()

    def issue_to(self, target):
        while self.issued < min(target, len(self.plan)):
            weight, half, hop = self.plan[self.issued]
            for way in (0, 1):
                if hop > 0:
                    self.arrive(weight, way if half is None else half, hop - 1, way)
                self.copy(self.issued, way).start()
            self.issued += 1

    def issue_share(self, numerator, denominator):
        self.issue_to(len(self.plan) * numerator // denominator)

    def issue_through(self, weight, hop):
        while any(w == weight and h <= hop for w, _, h in self.plan[self.issued :]):
            self.issue_to(self.issued + 1)

    def arrive_hop(self, weight, hop, way):
        for half in (0, 1):
            if (weight, half, hop, way) in self.number:
                self.arrive(weight, half, hop, way)

    def arrive_all(self, weight):
        for hop in range(self.count // 2):
            for way in (0, 1):
                self.arrive_hop(weight, hop, way)

    def finish(self):
        for at in range(len(self.plan)):
            for way in (0, 1):
                self.copy(at, way).wait_send()


class Group:
    def __init__(self, axis):
        self.axis = axis
        self.count = lax.axis_size(axis)
        self.me = lax.axis_index(axis)
        self.half = self.count // 2

    def device(self, offset, sibling):
        side = lax.rem(self.me, 2)
        group = lax.rem(self.me // 2 + offset + self.half, self.half)
        return 2 * group + (1 - side if sibling else side)

    def copy(self, source, target, sems, slot, device):
        return pltpu.make_async_remote_copy(
            src_ref=source,
            dst_ref=target,
            send_sem=sems[0].at[slot],
            recv_sem=sems[1].at[slot],
            device_id={self.axis: device},
            device_id_type=MESH,
        )


class Spread:
    def __init__(self, group, source, block, side_sems, far_sems, pass_sems):
        self.group, self.source, self.block = group, source, block
        self.side_sems, self.far_sems, self.pass_sems = side_sems, far_sems, pass_sems
        self.others = range(1, group.half)

    def slot(self, piece, offset):
        return piece * (self.group.half - 1) + offset - 1

    def side(self, piece):
        group = self.group
        return group.copy(
            self.source(piece), self.block(group.me, piece), self.side_sems, piece,
            group.device(0, True),
        )

    def far(self, piece, offset):
        group = self.group
        return group.copy(
            self.source(piece), self.block(group.me, piece), self.far_sems,
            self.slot(piece, offset), group.device(offset, False),
        )

    def onward(self, piece, offset):
        group = self.group
        block = self.block(group.device(-offset, False), piece)
        return group.copy(
            block, block, self.pass_sems, self.slot(piece, offset), group.device(0, True)
        )

    def start(self, piece):
        for offset in self.others:
            self.far(piece, offset).start()
        self.side(piece).start()

    def hand_on(self, piece):
        for offset in self.others:
            self.far(piece, offset).wait_recv()
            self.onward(piece, offset).start()

    def arrive(self, piece):
        self.side(piece).wait_recv()
        for offset in self.others:
            self.onward(piece, offset).wait_recv()

    def finish(self, piece):
        self.side(piece).wait_send()
        for offset in self.others:
            self.far(piece, offset).wait_send()
            self.onward(piece, offset).wait_send()


def layer_kernel(
    q_in, k_in, v_in, decay_in, rate_in, extra_in, out_gate_in, residual_in, out_weight_in,
    gate_in, up_in, down_in, head_gain, ffn_gain, taps,
    out,
    q, k, v, decay, rate, extra, out_gate, local, reach, state, maps, passed,
    stream, out_weight, mixed, normed, full_gate, full_up, full_down, hidden,
    part, near, leaving, far, result,
    load_sem, out_sem, ring_send, ring_recv, map_over_send, map_over_recv,
    map_across_send, map_across_recv, state_send, state_recv, halo_send, halo_recv,
    rows_side_send, rows_side_recv, rows_far_send, rows_far_recv, rows_pass_send, rows_pass_recv,
    wide_side_send, wide_side_recv, wide_far_send, wide_far_recv, wide_pass_send, wide_pass_recv,
    mix_side_send, mix_side_recv, mix_far_send, mix_far_recv, mix_pass_send, mix_pass_recv,
    near_send, near_recv, far_send, far_recv,
):
    tokens, width = q.shape
    features = stream.shape[1]
    group = Group("tp")
    around = lax.axis_size("sp")
    place = lax.axis_index("sp")
    own_rows = tokens // group.count
    ring = Ring(
        "sp", (gate_in, up_in, down_in), (full_gate, full_up, full_down), (ring_send, ring_recv)
    )
    shard = down_in.shape[0]

    def owned(ref, index, rows):
        return ref.at[pl.ds(pl.multiple_of(index * rows, rows), rows)]

    pairs = list(
        zip(
            (q_in, k_in, v_in, decay_in, rate_in, extra_in, out_gate_in),
            (q, k, v, decay, rate, extra, out_gate),
        )
    )
    inputs = len(pairs)
    pairs += [
        (residual_in, owned(stream, group.me, own_rows)),
        (out_weight_in, owned(out_weight, group.me, width)),
        (gate_in, owned(full_gate, place, shard)),
        (up_in, owned(full_up, place, shard)),
        (down_in, owned(full_down, place, shard)),
    ]
    loads = [
        pltpu.make_async_copy(source, target, load_sem.at[at])
        for at, (source, target) in enumerate(pairs)
    ]
    for load in loads[:inputs]:
        load.start()

    barrier = pltpu.get_barrier_semaphore()
    for axis, count, me in (("sp", around, place), ("tp", group.count, group.me)):
        for step in range(1, count):
            pl.semaphore_signal(
                barrier, inc=1, device_id={axis: lax.rem(me + step, count)}, device_id_type=MESH
            )
    pl.semaphore_wait(barrier, around + group.count - 2)

    ring.issue_share(6, 21)
    rows_spread = Spread(
        group,
        lambda piece: residual_in,
        lambda index, piece: owned(stream, index, own_rows),
        (rows_side_send, rows_side_recv),
        (rows_far_send, rows_far_recv),
        (rows_pass_send, rows_pass_recv),
    )
    wide_spread = Spread(
        group,
        lambda piece: out_weight_in,
        lambda index, piece: owned(out_weight, index, width),
        (wide_side_send, wide_side_recv),
        (wide_far_send, wide_far_recv),
        (wide_pass_send, wide_pass_recv),
    )
    rows_spread.start(0)
    wide_spread.start(0)
    for load in loads[inputs:]:
        load.start()
    for load in loads[:inputs]:
        load.wait()

    def before_step(index):
        @pl.when(index == tokens // (BLOCK * PER_STEP) - 1)
        def _():
            ring.issue_share(8, 21)

    recurrence((q, k, v, decay, rate, extra), local, reach, state, before_step)

    outer, line, side = around // 2, place // 2, lax.rem(place, 2)

    def map_copy(index, sems, slot, device):
        return pltpu.make_async_remote_copy(
            src_ref=maps.at[index],
            dst_ref=maps.at[index],
            send_sem=sems[0].at[slot],
            recv_sem=sems[1].at[slot],
            device_id={"sp": device},
            device_id_type=MESH,
        )

    def map_over(offset):
        target = lax.rem(line + offset, outer) * 2 + side
        return map_copy(place, (map_over_send, map_over_recv), offset - 1, target)

    def map_across(offset):
        held = lax.rem(line - offset + outer, outer) * 2 + side
        return map_copy(
            held, (map_across_send, map_across_recv), offset, line * 2 + 1 - side
        )

    states_on = pltpu.make_async_remote_copy(
        src_ref=passed.at[1],
        dst_ref=passed.at[0],
        send_sem=state_send,
        recv_sem=state_recv,
        device_id={"sp": lax.rem(line + 1, outer) * 2 + side},
        device_id_type=MESH,
    )
    last_line = line == outer - 1
    before_last = line == outer - 2

    maps[place] = collapsed(state[...]).astype(NARROW)
    for offset in range(1, outer):

        @pl.when(line + offset < outer - 1)
        def _():
            map_over(offset).start()

    @pl.when((side == 0) | before_last)
    def _():
        map_across(0).start()

    rows_spread.hand_on(0)
    wide_spread.hand_on(0)
    ring.issue_share(9, 21)
    for offset in range(1, outer):

        @pl.when((line >= offset) & (line < outer - 1))
        def _():
            map_over(offset).wait_recv()
            map_across(offset).start()

    ring.issue_share(11, 21)

    @pl.when((side == 1) | before_last)
    def _():
        map_across(0).wait_recv()

    for offset in range(1, outer):

        @pl.when((line >= offset) & (line < outer - 1))
        def _():
            map_across(offset).wait_recv()

    mask = head_mask(width).astype(NARROW)

    def enter(step, entering):
        found = maps[step]
        high, low = parts_of(entering, 2)
        after = (
            found[:, :width].astype(WIDE)
            + mul(found[:, width:], stacked(high, mask))
            + mul(found[:, width:], stacked(low, mask))
        )
        return after

    @pl.when(line < outer - 1)
    def _():
        passed[0] = lax.fori_loop(0, place, enter, jnp.zeros((HEAD_WIDTH, width), WIDE))

    @pl.when(before_last)
    def _():
        passed[1] = lax.fori_loop(place, 2 * outer - 2, enter, passed[0])
        states_on.start()

    ring.issue_share(12, 21)

    @pl.when(last_line)
    def _():
        states_on.wait_recv()
        passed[0] = lax.fori_loop(2 * line, place, enter, passed[0])

    state[:, :width] = stacked(passed[0], mask).astype(WIDE)

    pieces = group.count
    own_lanes = pl.ds(pl.multiple_of(group.me * width, width), width)

    def mixed_block(index, piece):
        rows = pl.ds(pl.multiple_of(piece * own_rows, own_rows), own_rows)
        return mixed.at[rows, pl.ds(pl.multiple_of(index * width, width), width)]

    mix_spread = Spread(
        group,
        lambda piece: mixed_block(group.me, piece),
        mixed_block,
        (mix_side_send, mix_side_recv),
        (mix_far_send, mix_far_recv),
        (mix_pass_send, mix_pass_recv),
    )

    def mix(piece, carry):
        rows = pl.ds(pl.multiple_of(piece * own_rows, own_rows), own_rows)
        readout = local[rows] + mul(reach[rows], state[:, :width])
        centered = readout - fine_left(readout, mask, 2) * (1.0 / HEAD_WIDTH)
        variance = fine_left(centered * centered, mask, 2) * (1.0 / HEAD_WIDTH)
        value = (
            centered
            * lax.rsqrt(variance + 0.00064)
            * head_gain[...]
            * out_gate[rows].astype(WIDE)
        )
        mixed[rows, own_lanes] = value.astype(NARROW)
        mix_spread.start(piece)
        return carry

    lax.fori_loop(0, pieces, mix, 0)
    ring.issue_share(13, 21)
    rows_spread.arrive(0)
    wide_spread.arrive(0)
    rows_spread.finish(0)
    wide_spread.finish(0)
    loads[inputs].wait()
    loads[inputs + 1].wait()

    def settle(piece, carry):
        @pl.when(piece < pieces)
        def _():
            mix_spread.hand_on(piece)

        @pl.when(piece > 0)
        def _():
            done = piece - 1
            mix_spread.arrive(done)
            rows = pl.ds(pl.multiple_of(done * own_rows, own_rows), own_rows)
            total = mul(mixed[rows], out_weight[...])
            kept = (stream[rows].astype(WIDE) + total).astype(NARROW)
            stream[rows] = kept
            kept = kept.astype(WIDE)
            scale = lax.rsqrt(jnp.mean(kept * kept, axis=-1, keepdims=True) + 1e-06)
            after = pl.ds(pl.multiple_of(HALO + done * own_rows, HALO), own_rows)
            normed[after] = (kept * scale * ffn_gain[...]).astype(NARROW)

        return carry

    lax.fori_loop(0, pieces + 1, settle, 0)

    halo = pltpu.make_async_remote_copy(
        src_ref=normed.at[pl.ds(tokens, HALO)],
        dst_ref=normed.at[pl.ds(0, HALO)],
        send_sem=halo_send,
        recv_sem=halo_recv,
        device_id={"sp": lax.rem(place + 1, around)},
        device_id_type=MESH,
    )

    @pl.when(place < around - 1)
    def _():
        halo.start()

    @pl.when(place == 0)
    def _():
        normed[:HALO] = jnp.zeros((HALO, features), NARROW)

    ring.issue_share(18, 21)

    @pl.when(place > 0)
    def _():
        halo.wait_recv()

    for weight in (0, 1):
        ring.arrive_all(weight)
        loads[inputs + 2 + weight].wait()

    def lift(piece, carry):
        start = pl.multiple_of(piece * own_rows, own_rows)
        rows = normed[pl.ds(start, own_rows + HALO)]
        mixes = []
        for way, weight in enumerate((full_gate, full_up)):
            held = mul(rows, weight[...]).astype(NARROW).astype(WIDE)
            tap = [taps[at][way : way + 1].astype(WIDE) for at in range(3)]
            mixes.append(
                tap[0] * held[HALO - 2 : -2] + tap[1] * held[HALO - 1 : -1] + tap[2] * held[HALO:]
            )
        hidden[pl.ds(start, own_rows)] = (jax.nn.silu(mixes[0]) * mixes[1]).astype(NARROW)

        @pl.when(piece == pieces // 2)
        def _():
            ring.issue_share(19, 21)

        return carry

    lax.fori_loop(0, pieces, lift, 0)
    ring.issue_share(20, 21)

    block = part.shape[2]
    blocks = part.shape[0]
    by_arrival = block == shard
    loads[inputs + 4].wait()
    if not by_arrival:
        ring.issue_to(len(ring.plan))
        ring.arrive_all(2)

    def lanes_of(at):
        if by_arrival:
            odd = lax.rem(at, 2)
            owner = ring.index((2 * odd - 1) * ((at + 1) // 2))
        else:
            owner = at
        return pl.ds(pl.multiple_of(owner * block, block), block)

    def quarter(device):
        return pl.ds(pl.multiple_of(device * own_rows, own_rows), own_rows)

    def near_copy(at, offset):
        return group.copy(
            part.at[at, quarter(group.device(offset, True))],
            near.at[at, offset],
            (near_send, near_recv),
            at * group.half + offset,
            group.device(0, True),
        )

    def far_copy(at, offset):
        return group.copy(
            leaving.at[at, offset - 1],
            far.at[at, offset - 1],
            (far_send, far_recv),
            at * (group.half - 1) + offset - 1,
            group.device(offset, False),
        )

    def out_copy(at):
        lanes = lanes_of(at)
        return pltpu.make_async_copy(result.at[:, lanes], out.at[:, lanes], out_sem.at[at])

    for offset in range(1, outer):

        @pl.when(line + offset < outer - 1)
        def _():
            map_over(offset).wait_send()

        @pl.when((line >= offset) & (line < outer - 1))
        def _():
            map_across(offset).wait_send()

    @pl.when((side == 0) | before_last)
    def _():
        map_across(0).wait_send()

    @pl.when(before_last)
    def _():
        states_on.wait_send()

    @pl.when(place < around - 1)
    def _():
        halo.wait_send()

    def drain(piece, carry):
        mix_spread.finish(piece)
        return carry

    lax.fori_loop(0, pieces, drain, 0)

    early = blocks - 3 if by_arrival else blocks

    def pass_on(done):
        for offset in range(1, group.half):
            near_copy(done, offset).wait_recv()
            mine = part[done, quarter(group.device(offset, False))].astype(WIDE)
            total = mine + near[done, offset].astype(WIDE)
            leaving[done, offset - 1] = total.astype(NARROW)
            far_copy(done, offset).start()

    def close(at, carry):
        @pl.when((at >= early) & (at <= blocks))
        def _():
            pass_on(at - 1)

        if by_arrival:
            for fixed in range(1, blocks):
                hop = (fixed + 1) // 2 - 1

                @pl.when(at == fixed)
                def _():
                    ring.issue_through(2, hop + 1)
                    if hop == around // 2 - 1:
                        ring.arrive_hop(2, hop, 0)
                        ring.arrive_hop(2, hop, 1)
                    else:
                        ring.arrive_hop(2, hop, way_of(fixed))

        @pl.when(at < blocks)
        def _():
            weight = full_down[lanes_of(at)]
            part[at] = mul(hidden[...], weight, ((1,), (1,))).astype(NARROW)
            for offset in list(range(1, group.half)) + [0]:
                near_copy(at, offset).start()

        @pl.when((at >= 1) & (at < early))
        def _():
            pass_on(at - 1)

        @pl.when(at >= LAG)
        def _():
            done = at - LAG
            near_copy(done, 0).wait_recv()
            own = quarter(group.me)
            total = part[done, own].astype(WIDE) + near[done, 0].astype(WIDE)
            for offset in range(1, group.half):
                far_copy(done, offset).wait_recv()
                total = total + far[done, offset - 1].astype(WIDE)
            lanes = lanes_of(done)
            result[:, lanes] = (stream[own, lanes].astype(WIDE) + total).astype(NARROW)
            out_copy(done).start()
            for offset in range(group.half):
                near_copy(done, offset).wait_send()
            for offset in range(1, group.half):
                far_copy(done, offset).wait_send()

        return carry

    lax.fori_loop(0, blocks + LAG, close, 0)

    ring.finish()

    def flush(at, carry):
        out_copy(at).wait()
        return carry

    lax.fori_loop(0, blocks, flush, 0)


def way_of(fixed):
    return 1 if fixed % 2 else 0


def layer(*arrays):
    (
        q, k, v, decay, rate, extra, out_gate, residual, out_weight, gate, up, down,
        head_gain, ffn_gain, taps,
    ) = arrays
    tokens, width = q.shape
    own_rows, features = residual.shape
    units = gate.shape[1]
    around, across = lax.axis_size("sp"), lax.axis_size("tp")
    shard = down.shape[0]
    block = shard if shard % 128 == 0 else 256
    blocks = features // block
    half = across // 2
    others = half - 1
    entries = 2 * len(ring_plan(around))
    dma = pltpu.SemaphoreType.DMA

    def two(count):
        return [dma((count,)), dma((count,))]

    def vmem(*shape, dtype=NARROW):
        return pltpu.VMEM(shape, dtype)

    anywhere = pl.BlockSpec(memory_space=pl.ANY)
    near_by = pl.BlockSpec(memory_space=pltpu.VMEM)
    return pl.pallas_call(
        layer_kernel,
        in_specs=[anywhere] * 12 + [near_by] * 3,
        out_specs=anywhere,
        out_shape=jax.ShapeDtypeStruct((own_rows, features), NARROW),
        scratch_shapes=[vmem(tokens, width)] * 5
        + [
            vmem(tokens, width, dtype=WIDE),
            vmem(tokens, width),
            vmem(tokens, width, dtype=WIDE),
            vmem(tokens, width, dtype=WIDE),
            vmem(width, 2 * width, dtype=WIDE),
            vmem(around, HEAD_WIDTH, 2 * width),
            vmem(2, HEAD_WIDTH, width, dtype=WIDE),
            vmem(tokens, features),
            vmem(across * width, features),
            vmem(tokens, across * width),
            vmem(HALO + tokens, features),
            vmem(features, units),
            vmem(features, units),
            vmem(features, units),
            vmem(tokens, units),
            vmem(blocks, tokens, block),
            vmem(blocks, half, own_rows, block),
            vmem(blocks, others, own_rows, block),
            vmem(blocks, others, own_rows, block),
            vmem(own_rows, features),
            dma((12,)),
            dma((blocks,)),
        ]
        + two(entries)
        + two(around // 2 - 1)
        + two(around // 2)
        + [dma] * 4
        + (two(1) + two(others) + two(others)) * 2
        + two(across) + two(across * others) + two(across * others)
        + two(blocks * half)
        + two(blocks * others),
        compiler_params=pltpu.CompilerParams(
            collective_id=1, has_side_effects=True, vmem_limit_bytes=67043328
        ),
        name="layer",
    )(
        q, k, v, decay, rate, extra, out_gate, residual, out_weight, gate, up, down,
        head_gain[None], ffn_gain[None], taps,
    )


def body(
    residual_input_stream,
    receptance,
    key_matrix_all,
    value_matrix_all,
    decay_preactivation,
    learning_rate_preactivation,
    output_gate_all_heads,
    extra_log_decay,
    head_norm_gain,
    output_projection_weight,
    feedforward_norm_gain,
    gate_projection_weight,
    up_projection_weight,
    down_projection_weight,
    convolution_kernel,
):
    return layer(
        receptance,
        key_matrix_all,
        value_matrix_all,
        decay_preactivation,
        learning_rate_preactivation,
        extra_log_decay,
        output_gate_all_heads,
        residual_input_stream,
        output_projection_weight,
        gate_projection_weight,
        up_projection_weight,
        down_projection_weight,
        head_norm_gain,
        feedforward_norm_gain,
        convolution_kernel,
    )


def solution(mesh):
    in_specs = (
        P(("sp", "tp"), None),
        P("sp", "tp"),
        P("sp", "tp"),
        P("sp", "tp"),
        P("sp", "tp"),
        P("sp", "tp"),
        P("sp", "tp"),
        P("sp", "tp"),
        P("tp"),
        P("tp", None),
        P(),
        P("sp", "tp"),
        P("sp", "tp"),
        P("sp", "tp"),
        P(None, None, "tp"),
    )
    out_specs = P(("sp", "tp"), None)
    return jax.shard_map(
        body, mesh=mesh, in_specs=in_specs, out_specs=out_specs, check_vma=False
    )
```

```python
import functools

import jax
import jax.numpy as jnp
from jax import lax
from jax.experimental import pallas as pl
from jax.experimental.pallas import tpu as pltpu
from jax.sharding import PartitionSpec as P

HEAD_WIDTH = 64
BLOCK = 64
PER_STEP = 4
HALO = 16
LAG = 3
MESH = pl.DeviceIdType.MESH
WIDE = jnp.float32
NARROW = jnp.bfloat16


def mul(a, b, dims=((1,), (0,))):
    return lax.dot_general(
        a.astype(NARROW), b.astype(NARROW), (dims, ((), ())), preferred_element_type=WIDE
    )


def parts_of(a, count):
    found = []
    for _ in range(count):
        piece = a.astype(NARROW)
        found.append(piece)
        a = a - piece.astype(WIDE)
    return found


def fine_left(a, b, count, dims=((1,), (0,))):
    return sum(mul(piece, b, dims) for piece in parts_of(a, count))


def fine_right(a, b, count, dims=((1,), (0,))):
    return sum(mul(a, piece, dims) for piece in parts_of(b, count))


def head_mask(width):
    rows = lax.broadcasted_iota(jnp.int32, (width, width), 0) // HEAD_WIDTH
    lanes = lax.broadcasted_iota(jnp.int32, (width, width), 1) // HEAD_WIDTH
    return jnp.where(rows == lanes, 1.0, 0.0)


def stacked(a, mask):
    a = a.astype(NARROW)
    return jnp.concatenate([a] * (mask.shape[0] // a.shape[0]), axis=0) * mask


def fine_product(a, b, mask):
    a_high, a_low = parts_of(a, 2)
    b_high, b_low = (stacked(piece, mask) for piece in parts_of(b, 2))
    return mul(a_high, b_high) + mul(a_low, b_high) + mul(a_high, b_low)


def collapsed(a):
    heads = a.shape[0] // HEAD_WIDTH
    return sum(a[h * HEAD_WIDTH : (h + 1) * HEAD_WIDTH] for h in range(heads))


def recurrence(refs, local_ref, reach_ref, state, before_step):
    q_ref, k_ref, v_ref, decay_ref, rate_ref, extra_ref = refs
    tokens, width = q_ref.shape
    mask_wide = head_mask(width)
    mask = mask_wide.astype(NARROW)
    last = ((1,), (1,))
    first = ((0,), (0,))

    rows = lax.broadcasted_iota(jnp.int32, (width, width), 0)
    lanes = lax.broadcasted_iota(jnp.int32, (width, width), 1)
    state[:, :width] = jnp.zeros((width, width), WIDE)
    state[:, width:] = jnp.where(rows == lanes, 1.0, 0.0)

    def one(index, carry):
        before_step(index)
        token = lax.broadcasted_iota(jnp.int32, (BLOCK, width), 0)
        other = lax.broadcasted_iota(jnp.int32, (BLOCK, width), 1) % BLOCK
        strict = token > other
        within = token >= other
        eye = jnp.where(token == other, 1.0, 0.0)
        lower = jnp.where(
            lax.broadcasted_iota(jnp.int32, (BLOCK, BLOCK), 0)
            >= lax.broadcasted_iota(jnp.int32, (BLOCK, BLOCK), 1),
            1.0,
            0.0,
        ).astype(NARROW)
        ones = jnp.ones((BLOCK, width), NARROW)

        def window(part):
            return pl.ds(pl.multiple_of((index * PER_STEP + part) * BLOCK, BLOCK), BLOCK)

        prepared = []
        for part in range(PER_STEP):
            at = window(part)
            q = q_ref[at].astype(WIDE)
            k = k_ref[at].astype(WIDE)
            v = stacked(v_ref[at], mask)
            log_decay = (
                -jnp.exp(-0.5) * jax.nn.sigmoid(decay_ref[at].astype(WIDE)) + extra_ref[at]
            )
            rates = jax.nn.sigmoid(rate_ref[at].astype(WIDE))
            normed = k * lax.rsqrt(fine_left(k * k, mask, 2) + 1e-06)
            removal = normed * rates
            cum = fine_right(lower, log_decay, 3)
            previous = cum - log_decay
            middle = cum[BLOCK // 2 : BLOCK // 2 + 1]
            end = cum[BLOCK - 1 : BLOCK]
            back = jnp.exp(middle - cum)
            left = jnp.concatenate(
                [normed * jnp.exp(previous - middle), q * jnp.exp(cum - middle)], axis=0
            )
            by_key = mul(left, stacked(k * back, mask), last)
            by_removal = mul(left, stacked(removal * back, mask), last)
            key_rate = jnp.where(strict, by_key[:BLOCK], 0.0)
            removal_rate = jnp.where(strict, by_removal[:BLOCK], 0.0)
            key_out = jnp.where(within, by_key[BLOCK:], 0.0)
            removal_out = jnp.where(within, by_removal[BLOCK:], 0.0)
            inverse = eye
            size = 1
            while size < BLOCK:
                pair = (token // (2 * size) == other // (2 * size)) & (
                    token // size != other // size
                )
                piece = jnp.where(pair, removal_rate, 0.0)
                if size == 1:
                    inverse = inverse - piece
                else:
                    inverse = inverse - fine_product(
                        fine_product(inverse, piece, mask), inverse, mask
                    )
                size *= 2
            from_state = mul(inverse, stacked(normed * jnp.exp(previous), mask))
            keyed = mul(jnp.concatenate([key_rate, key_out], axis=0), v)
            offset = mul(inverse, stacked(keyed[:BLOCK], mask))
            reach = q * jnp.exp(cum) - mul(removal_out, stacked(from_state, mask))
            local = keyed[BLOCK:] - mul(removal_out, stacked(offset, mask))
            to_end = jnp.exp(end - cum)
            span = jnp.exp(fine_left(log_decay, ones, 3, first))
            prepared.append((from_state, offset, reach, local, k * to_end, removal * to_end, span))

        for part in range(PER_STEP):
            at = window(part)
            from_state, offset, reach, local, key_end, removal_end, span = prepared[part]
            now = state[...]
            both = mul(jnp.concatenate([from_state, reach], axis=0), now)
            correction = both[:BLOCK, :width] + offset
            local_ref[at] = local + both[BLOCK:, :width]
            reach_ref[at] = both[BLOCK:, width:]
            kept_value = mul(
                jnp.concatenate([key_end, -removal_end], axis=0),
                jnp.concatenate([v_ref[at].astype(WIDE), correction], axis=0),
                first,
            )
            kept_map = mul(-removal_end, both[:BLOCK, width:], first)
            state[:, :width] = now[:, :width] * span + kept_value * mask_wide
            state[:, width:] = now[:, width:] * span + kept_map * mask_wide
        return carry

    lax.fori_loop(0, tokens // (BLOCK * PER_STEP), one, 0)


def ring_plan(count):
    hops = count // 2

    def entries(weight, hop):
        if hop < hops - 1:
            return [(weight, 0, hop), (weight, 1, hop)]
        return [(weight, None, hop)]

    plan = []
    for weight in range(3):
        plan += entries(weight, 0)
    for hop in range(1, hops):
        plan += entries(0, hop) + entries(1, hop)
    for hop in range(1, hops):
        plan += entries(2, hop)
    return plan


class Ring:
    def __init__(self, axis, shards, gathered, sems):
        self.axis, self.shards, self.gathered, self.sems = axis, shards, gathered, sems
        self.count = lax.axis_size(axis)
        me = lax.axis_index(axis)
        odd = lax.rem(me, 2)
        self.place = (1 - odd) * (me // 2) + odd * (self.count - 1 - me // 2)
        self.plan = ring_plan(self.count)
        self.number = {}
        for at, (weight, half, hop) in enumerate(self.plan):
            for way in (0, 1):
                self.number[weight, way if half is None else half, hop, way] = at
        self.issued = 0
        self.waited = set()

    def index(self, offset):
        at = lax.rem(self.place + offset + 2 * self.count, self.count)
        upper = at // (self.count // 2)
        return (1 - upper) * 2 * at + upper * (2 * (self.count - 1 - at) + 1)

    def block(self, weight, half, offset):
        rows = self.shards[weight].shape[0]
        start = self.index(offset) * rows + half * (rows // 2)
        return self.gathered[weight].at[pl.ds(pl.multiple_of(start, rows // 2), rows // 2)]

    def copy(self, at, way):
        weight, half, hop = self.plan[at]
        half = way if half is None else half
        rows = self.shards[weight].shape[0] // 2
        back = -hop if way == 0 else hop
        target = self.block(weight, half, back)
        source = self.shards[weight].at[pl.ds(half * rows, rows)] if hop == 0 else target
        slot = 2 * at + way
        return pltpu.make_async_remote_copy(
            src_ref=source,
            dst_ref=target,
            send_sem=self.sems[0].at[slot],
            recv_sem=self.sems[1].at[slot],
            device_id={self.axis: self.index(1 if way == 0 else -1)},
            device_id_type=MESH,
        )

    def arrive(self, weight, half, hop, way):
        at = self.number[weight, half, hop, way]
        if (at, way) not in self.waited:
            self.waited.add((at, way))
            self.copy(at, way).wait_recv()

    def issue_to(self, target):
        while self.issued < min(target, len(self.plan)):
            weight, half, hop = self.plan[self.issued]
            for way in (0, 1):
                if hop > 0:
                    self.arrive(weight, way if half is None else half, hop - 1, way)
                self.copy(self.issued, way).start()
            self.issued += 1

    def issue_share(self, numerator, denominator):
        self.issue_to(len(self.plan) * numerator // denominator)

    def issue_through(self, weight, hop):
        while any(w == weight and h <= hop for w, _, h in self.plan[self.issued :]):
            self.issue_to(self.issued + 1)

    def arrive_hop(self, weight, hop, way):
        for half in (0, 1):
            if (weight, half, hop, way) in self.number:
                self.arrive(weight, half, hop, way)

    def arrive_all(self, weight):
        for hop in range(self.count // 2):
            for way in (0, 1):
                self.arrive_hop(weight, hop, way)

    def finish(self):
        for at in range(len(self.plan)):
            for way in (0, 1):
                self.copy(at, way).wait_send()


class Group:
    def __init__(self, axis):
        self.axis = axis
        self.count = lax.axis_size(axis)
        self.me = lax.axis_index(axis)
        self.half = self.count // 2

    def device(self, offset, sibling):
        side = lax.rem(self.me, 2)
        group = lax.rem(self.me // 2 + offset + self.half, self.half)
        return 2 * group + (1 - side if sibling else side)

    def copy(self, source, target, sems, slot, device):
        return pltpu.make_async_remote_copy(
            src_ref=source,
            dst_ref=target,
            send_sem=sems[0].at[slot],
            recv_sem=sems[1].at[slot],
            device_id={self.axis: device},
            device_id_type=MESH,
        )


class Spread:
    def __init__(self, group, source, block, side_sems, far_sems, pass_sems):
        self.group, self.source, self.block = group, source, block
        self.side_sems, self.far_sems, self.pass_sems = side_sems, far_sems, pass_sems
        self.others = range(1, group.half)

    def slot(self, piece, offset):
        return piece * (self.group.half - 1) + offset - 1

    def side(self, piece):
        group = self.group
        return group.copy(
            self.source(piece), self.block(group.me, piece), self.side_sems, piece,
            group.device(0, True),
        )

    def far(self, piece, offset):
        group = self.group
        return group.copy(
            self.source(piece), self.block(group.me, piece), self.far_sems,
            self.slot(piece, offset), group.device(offset, False),
        )

    def onward(self, piece, offset):
        group = self.group
        block = self.block(group.device(-offset, False), piece)
        return group.copy(
            block, block, self.pass_sems, self.slot(piece, offset), group.device(0, True)
        )

    def start(self, piece):
        for offset in self.others:
            self.far(piece, offset).start()
        self.side(piece).start()

    def hand_on(self, piece):
        for offset in self.others:
            self.far(piece, offset).wait_recv()
            self.onward(piece, offset).start()

    def arrive(self, piece):
        self.side(piece).wait_recv()
        for offset in self.others:
            self.onward(piece, offset).wait_recv()

    def finish(self, piece):
        self.side(piece).wait_send()
        for offset in self.others:
            self.far(piece, offset).wait_send()
            self.onward(piece, offset).wait_send()


def layer_kernel(
    q_in, k_in, v_in, decay_in, rate_in, extra_in, out_gate_in, residual_in, out_weight_in,
    gate_in, up_in, down_in, head_gain, ffn_gain, taps,
    out,
    q, k, v, decay, rate, extra, out_gate, local, reach, state, maps, passed,
    stream, out_weight, mixed, normed, full_gate, full_up, full_down, hidden,
    part, near, leaving, far, result,
    load_sem, out_sem, ring_send, ring_recv, map_over_send, map_over_recv,
    map_across_send, map_across_recv, state_send, state_recv, halo_send, halo_recv,
    rows_side_send, rows_side_recv, rows_far_send, rows_far_recv, rows_pass_send, rows_pass_recv,
    wide_side_send, wide_side_recv, wide_far_send, wide_far_recv, wide_pass_send, wide_pass_recv,
    mix_side_send, mix_side_recv, mix_far_send, mix_far_recv, mix_pass_send, mix_pass_recv,
    near_send, near_recv, far_send, far_recv,
):
    tokens, width = q.shape
    features = stream.shape[1]
    group = Group("tp")
    around = lax.axis_size("sp")
    place = lax.axis_index("sp")
    own_rows = tokens // group.count
    ring = Ring(
        "sp", (gate_in, up_in, down_in), (full_gate, full_up, full_down), (ring_send, ring_recv)
    )
    shard = down_in.shape[0]

    def owned(ref, index, rows):
        return ref.at[pl.ds(pl.multiple_of(index * rows, rows), rows)]

    pairs = list(
        zip(
            (q_in, k_in, v_in, decay_in, rate_in, extra_in, out_gate_in),
            (q, k, v, decay, rate, extra, out_gate),
        )
    )
    inputs = len(pairs)
    pairs += [
        (residual_in, owned(stream, group.me, own_rows)),
        (out_weight_in, owned(out_weight, group.me, width)),
        (gate_in, owned(full_gate, place, shard)),
        (up_in, owned(full_up, place, shard)),
        (down_in, owned(full_down, place, shard)),
    ]
    loads = [
        pltpu.make_async_copy(source, target, load_sem.at[at])
        for at, (source, target) in enumerate(pairs)
    ]
    for load in loads[:inputs]:
        load.start()

    barrier = pltpu.get_barrier_semaphore()
    for axis, count, me in (("sp", around, place), ("tp", group.count, group.me)):
        for step in range(1, count):
            pl.semaphore_signal(
                barrier, inc=1, device_id={axis: lax.rem(me + step, count)}, device_id_type=MESH
            )
    pl.semaphore_wait(barrier, around + group.count - 2)

    ring.issue_share(6, 21)
    rows_spread = Spread(
        group,
        lambda piece: residual_in,
        lambda index, piece: owned(stream, index, own_rows),
        (rows_side_send, rows_side_recv),
        (rows_far_send, rows_far_recv),
        (rows_pass_send, rows_pass_recv),
    )
    wide_spread = Spread(
        group,
        lambda piece: out_weight_in,
        lambda index, piece: owned(out_weight, index, width),
        (wide_side_send, wide_side_recv),
        (wide_far_send, wide_far_recv),
        (wide_pass_send, wide_pass_recv),
    )
    rows_spread.start(0)
    wide_spread.start(0)
    for load in loads[inputs:]:
        load.start()
    for load in loads[:inputs]:
        load.wait()

    def before_step(index):
        @pl.when(index == tokens // (BLOCK * PER_STEP) - 1)
        def _():
            ring.issue_share(8, 21)

    recurrence((q, k, v, decay, rate, extra), local, reach, state, before_step)

    outer, line, side = around // 2, place // 2, lax.rem(place, 2)

    def map_copy(index, sems, slot, device):
        return pltpu.make_async_remote_copy(
            src_ref=maps.at[index],
            dst_ref=maps.at[index],
            send_sem=sems[0].at[slot],
            recv_sem=sems[1].at[slot],
            device_id={"sp": device},
            device_id_type=MESH,
        )

    def map_over(offset):
        target = lax.rem(line + offset, outer) * 2 + side
        return map_copy(place, (map_over_send, map_over_recv), offset - 1, target)

    def map_across(offset):
        held = lax.rem(line - offset + outer, outer) * 2 + side
        return map_copy(
            held, (map_across_send, map_across_recv), offset, line * 2 + 1 - side
        )

    states_on = pltpu.make_async_remote_copy(
        src_ref=passed.at[1],
        dst_ref=passed.at[0],
        send_sem=state_send,
        recv_sem=state_recv,
        device_id={"sp": lax.rem(line + 1, outer) * 2 + side},
        device_id_type=MESH,
    )
    last_line = line == outer - 1
    before_last = line == outer - 2

    maps[place] = collapsed(state[...]).astype(NARROW)
    for offset in range(1, outer):

        @pl.when(line + offset < outer - 1)
        def _():
            map_over(offset).start()

    @pl.when((side == 0) | before_last)
    def _():
        map_across(0).start()

    rows_spread.hand_on(0)
    wide_spread.hand_on(0)
    ring.issue_share(9, 21)
    for offset in range(1, outer):

        @pl.when((line >= offset) & (line < outer - 1))
        def _():
            map_over(offset).wait_recv()
            map_across(offset).start()

    ring.issue_share(11, 21)

    @pl.when((side == 1) | before_last)
    def _():
        map_across(0).wait_recv()

    for offset in range(1, outer):

        @pl.when((line >= offset) & (line < outer - 1))
        def _():
            map_across(offset).wait_recv()

    mask = head_mask(width).astype(NARROW)

    def enter(step, entering):
        found = maps[step]
        high, low = parts_of(entering, 2)
        after = (
            found[:, :width].astype(WIDE)
            + mul(found[:, width:], stacked(high, mask))
            + mul(found[:, width:], stacked(low, mask))
        )
        return after

    @pl.when(line < outer - 1)
    def _():
        passed[0] = lax.fori_loop(0, place, enter, jnp.zeros((HEAD_WIDTH, width), WIDE))

    @pl.when(before_last)
    def _():
        passed[1] = lax.fori_loop(place, 2 * outer - 2, enter, passed[0])
        states_on.start()

    ring.issue_share(12, 21)

    @pl.when(last_line)
    def _():
        states_on.wait_recv()
        passed[0] = lax.fori_loop(2 * line, place, enter, passed[0])

    state[:, :width] = stacked(passed[0], mask).astype(WIDE)

    pieces = group.count
    own_lanes = pl.ds(pl.multiple_of(group.me * width, width), width)

    def mixed_block(index, piece):
        rows = pl.ds(pl.multiple_of(piece * own_rows, own_rows), own_rows)
        return mixed.at[rows, pl.ds(pl.multiple_of(index * width, width), width)]

    mix_spread = Spread(
        group,
        lambda piece: mixed_block(group.me, piece),
        mixed_block,
        (mix_side_send, mix_side_recv),
        (mix_far_send, mix_far_recv),
        (mix_pass_send, mix_pass_recv),
    )

    def mix(piece, carry):
        rows = pl.ds(pl.multiple_of(piece * own_rows, own_rows), own_rows)
        readout = local[rows] + mul(reach[rows], state[:, :width])
        centered = readout - fine_left(readout, mask, 2) * (1.0 / HEAD_WIDTH)
        variance = fine_left(centered * centered, mask, 2) * (1.0 / HEAD_WIDTH)
        value = (
            centered
            * lax.rsqrt(variance + 0.00064)
            * head_gain[...]
            * out_gate[rows].astype(WIDE)
        )
        mixed[rows, own_lanes] = value.astype(NARROW)
        mix_spread.start(piece)
        return carry

    lax.fori_loop(0, pieces, mix, 0)
    ring.issue_share(13, 21)
    rows_spread.arrive(0)
    wide_spread.arrive(0)
    rows_spread.finish(0)
    wide_spread.finish(0)
    loads[inputs].wait()
    loads[inputs + 1].wait()

    def settle(piece, carry):
        @pl.when(piece < pieces)
        def _():
            mix_spread.hand_on(piece)

        @pl.when(piece > 0)
        def _():
            done = piece - 1
            mix_spread.arrive(done)
            rows = pl.ds(pl.multiple_of(done * own_rows, own_rows), own_rows)
            total = mul(mixed[rows], out_weight[...])
            kept = (stream[rows].astype(WIDE) + total).astype(NARROW)
            stream[rows] = kept
            kept = kept.astype(WIDE)
            scale = lax.rsqrt(jnp.mean(kept * kept, axis=-1, keepdims=True) + 1e-06)
            after = pl.ds(pl.multiple_of(HALO + done * own_rows, HALO), own_rows)
            normed[after] = (kept * scale * ffn_gain[...]).astype(NARROW)

        return carry

    lax.fori_loop(0, pieces + 1, settle, 0)

    halo = pltpu.make_async_remote_copy(
        src_ref=normed.at[pl.ds(tokens, HALO)],
        dst_ref=normed.at[pl.ds(0, HALO)],
        send_sem=halo_send,
        recv_sem=halo_recv,
        device_id={"sp": lax.rem(place + 1, around)},
        device_id_type=MESH,
    )

    @pl.when(place < around - 1)
    def _():
        halo.start()

    @pl.when(place == 0)
    def _():
        normed[:HALO] = jnp.zeros((HALO, features), NARROW)

    ring.issue_share(18, 21)

    @pl.when(place > 0)
    def _():
        halo.wait_recv()

    for weight in (0, 1):
        ring.arrive_all(weight)
        loads[inputs + 2 + weight].wait()

    def lift(piece, carry):
        start = pl.multiple_of(piece * own_rows, own_rows)
        rows = normed[pl.ds(start, own_rows + HALO)]
        mixes = []
        for way, weight in enumerate((full_gate, full_up)):
            held = mul(rows, weight[...]).astype(NARROW).astype(WIDE)
            tap = [taps[at][way : way + 1].astype(WIDE) for at in range(3)]
            mixes.append(
                tap[0] * held[HALO - 2 : -2] + tap[1] * held[HALO - 1 : -1] + tap[2] * held[HALO:]
            )
        hidden[pl.ds(start, own_rows)] = (jax.nn.silu(mixes[0]) * mixes[1]).astype(NARROW)

        @pl.when(piece == pieces // 2)
        def _():
            ring.issue_share(19, 21)

        return carry

    lax.fori_loop(0, pieces, lift, 0)
    ring.issue_share(20, 21)

    block = part.shape[2]
    blocks = part.shape[0]
    by_arrival = block == shard
    loads[inputs + 4].wait()
    if not by_arrival:
        ring.issue_to(len(ring.plan))
        ring.arrive_all(2)

    def lanes_of(at):
        if by_arrival:
            odd = lax.rem(at, 2)
            owner = ring.index((2 * odd - 1) * ((at + 1) // 2))
        else:
            owner = at
        return pl.ds(pl.multiple_of(owner * block, block), block)

    def quarter(device):
        return pl.ds(pl.multiple_of(device * own_rows, own_rows), own_rows)

    def near_copy(at, offset):
        return group.copy(
            part.at[at, quarter(group.device(offset, True))],
            near.at[at, offset],
            (near_send, near_recv),
            at * group.half + offset,
            group.device(0, True),
        )

    def far_copy(at, offset):
        return group.copy(
            leaving.at[at, offset - 1],
            far.at[at, offset - 1],
            (far_send, far_recv),
            at * (group.half - 1) + offset - 1,
            group.device(offset, False),
        )

    def out_copy(at):
        lanes = lanes_of(at)
        return pltpu.make_async_copy(result.at[:, lanes], out.at[:, lanes], out_sem.at[at])

    for offset in range(1, outer):

        @pl.when(line + offset < outer - 1)
        def _():
            map_over(offset).wait_send()

        @pl.when((line >= offset) & (line < outer - 1))
        def _():
            map_across(offset).wait_send()

    @pl.when((side == 0) | before_last)
    def _():
        map_across(0).wait_send()

    @pl.when(before_last)
    def _():
        states_on.wait_send()

    @pl.when(place < around - 1)
    def _():
        halo.wait_send()

    def drain(piece, carry):
        mix_spread.finish(piece)
        return carry

    lax.fori_loop(0, pieces, drain, 0)

    early = blocks - 3 if by_arrival else blocks

    def pass_on(done):
        for offset in range(1, group.half):
            near_copy(done, offset).wait_recv()
            mine = part[done, quarter(group.device(offset, False))].astype(WIDE)
            total = mine + near[done, offset].astype(WIDE)
            leaving[done, offset - 1] = total.astype(NARROW)
            far_copy(done, offset).start()

    def close(at, carry):
        @pl.when((at >= early) & (at <= blocks))
        def _():
            pass_on(at - 1)

        if by_arrival:
            for fixed in range(1, blocks):
                hop = (fixed + 1) // 2 - 1

                @pl.when(at == fixed)
                def _():
                    ring.issue_through(2, hop + 1)
                    if hop == around // 2 - 1:
                        ring.arrive_hop(2, hop, 0)
                        ring.arrive_hop(2, hop, 1)
                    else:
                        ring.arrive_hop(2, hop, way_of(fixed))

        @pl.when(at < blocks)
        def _():
            weight = full_down[lanes_of(at)]
            both = 2 * own_rows
            for offset in list(range(1, group.half)) + [0]:
                chip = group.device(offset, False) // 2
                rows = pl.ds(pl.multiple_of(chip * both, both), both)
                part[at, rows] = mul(hidden[rows], weight, ((1,), (1,))).astype(NARROW)
                near_copy(at, offset).start()

        @pl.when((at >= 1) & (at < early))
        def _():
            pass_on(at - 1)

        @pl.when(at >= LAG)
        def _():
            done = at - LAG
            near_copy(done, 0).wait_recv()
            own = quarter(group.me)
            total = part[done, own].astype(WIDE) + near[done, 0].astype(WIDE)
            for offset in range(1, group.half):
                far_copy(done, offset).wait_recv()
                total = total + far[done, offset - 1].astype(WIDE)
            lanes = lanes_of(done)
            result[:, lanes] = (stream[own, lanes].astype(WIDE) + total).astype(NARROW)
            out_copy(done).start()
            for offset in range(group.half):
                near_copy(done, offset).wait_send()
            for offset in range(1, group.half):
                far_copy(done, offset).wait_send()

        return carry

    lax.fori_loop(0, blocks + LAG, close, 0)

    ring.finish()

    def flush(at, carry):
        out_copy(at).wait()
        return carry

    lax.fori_loop(0, blocks, flush, 0)


def way_of(fixed):
    return 1 if fixed % 2 else 0


def layer(*arrays):
    (
        q, k, v, decay, rate, extra, out_gate, residual, out_weight, gate, up, down,
        head_gain, ffn_gain, taps,
    ) = arrays
    tokens, width = q.shape
    own_rows, features = residual.shape
    units = gate.shape[1]
    around, across = lax.axis_size("sp"), lax.axis_size("tp")
    shard = down.shape[0]
    block = shard if shard % 128 == 0 else 256
    blocks = features // block
    half = across // 2
    others = half - 1
    entries = 2 * len(ring_plan(around))
    dma = pltpu.SemaphoreType.DMA

    def two(count):
        return [dma((count,)), dma((count,))]

    def vmem(*shape, dtype=NARROW):
        return pltpu.VMEM(shape, dtype)

    anywhere = pl.BlockSpec(memory_space=pl.ANY)
    near_by = pl.BlockSpec(memory_space=pltpu.VMEM)
    return pl.pallas_call(
        layer_kernel,
        in_specs=[anywhere] * 12 + [near_by] * 3,
        out_specs=anywhere,
        out_shape=jax.ShapeDtypeStruct((own_rows, features), NARROW),
        scratch_shapes=[vmem(tokens, width)] * 5
        + [
            vmem(tokens, width, dtype=WIDE),
            vmem(tokens, width),
            vmem(tokens, width, dtype=WIDE),
            vmem(tokens, width, dtype=WIDE),
            vmem(width, 2 * width, dtype=WIDE),
            vmem(around, HEAD_WIDTH, 2 * width),
            vmem(2, HEAD_WIDTH, width, dtype=WIDE),
            vmem(tokens, features),
            vmem(across * width, features),
            vmem(tokens, across * width),
            vmem(HALO + tokens, features),
            vmem(features, units),
            vmem(features, units),
            vmem(features, units),
            vmem(tokens, units),
            vmem(blocks, tokens, block),
            vmem(blocks, half, own_rows, block),
            vmem(blocks, others, own_rows, block),
            vmem(blocks, others, own_rows, block),
            vmem(own_rows, features),
            dma((12,)),
            dma((blocks,)),
        ]
        + two(entries)
        + two(around // 2 - 1)
        + two(around // 2)
        + [dma] * 4
        + (two(1) + two(others) + two(others)) * 2
        + two(across) + two(across * others) + two(across * others)
        + two(blocks * half)
        + two(blocks * others),
        compiler_params=pltpu.CompilerParams(
            collective_id=1, has_side_effects=True, vmem_limit_bytes=67043328
        ),
        name="layer",
    )(
        q, k, v, decay, rate, extra, out_gate, residual, out_weight, gate, up, down,
        head_gain[None], ffn_gain[None], taps,
    )


def body(
    residual_input_stream,
    receptance,
    key_matrix_all,
    value_matrix_all,
    decay_preactivation,
    learning_rate_preactivation,
    output_gate_all_heads,
    extra_log_decay,
    head_norm_gain,
    output_projection_weight,
    feedforward_norm_gain,
    gate_projection_weight,
    up_projection_weight,
    down_projection_weight,
    convolution_kernel,
):
    return layer(
        receptance,
        key_matrix_all,
        value_matrix_all,
        decay_preactivation,
        learning_rate_preactivation,
        extra_log_decay,
        output_gate_all_heads,
        residual_input_stream,
        output_projection_weight,
        gate_projection_weight,
        up_projection_weight,
        down_projection_weight,
        head_norm_gain,
        feedforward_norm_gain,
        convolution_kernel,
    )


def solution(mesh):
    in_specs = (
        P(("sp", "tp"), None),
        P("sp", "tp"),
        P("sp", "tp"),
        P("sp", "tp"),
        P("sp", "tp"),
        P("sp", "tp"),
        P("sp", "tp"),
        P("sp", "tp"),
        P("tp"),
        P("tp", None),
        P(),
        P("sp", "tp"),
        P("sp", "tp"),
        P("sp", "tp"),
        P(None, None, "tp"),
    )
    out_specs = P(("sp", "tp"), None)
    return jax.shard_map(
        body, mesh=mesh, in_specs=in_specs, out_specs=out_specs, check_vma=False
    )
```
